128 devices in a mesh: rep: 2 (over z_hi), fs: 32 (over z_lo, y, x), tp: 2 (over core).
Axes of the slice: x: 4, y: 4, z: 4 (z_hi: 2, z_lo: 2; z = z_hi * 2 + z_lo), core: 2. Of those that a mesh axis runs over, the one named last changes fastest.
Arguments:
- stream_in: bfloat16 [64, 768, 2048], P(('rep', 'fs'), None, 'tp'), may hold values from -6 to 6
- mix_gain: float32 [2048], replicated, may hold values from 0.1 to 1.9
- lin_weight: bfloat16 [2048, 2048], P('fs', 'tp'), may hold values from -0.125 to 0.125
- branch_weight: bfloat16 [2048, 2048], P('fs', 'tp'), may hold values from -0.125 to 0.125
- lin_taps: float32 [4, 2048], P(None, 'tp'), may hold values from -3 to 3
- rate_blocks: bfloat16 [16, 128, 128], P('tp'), may hold values from -0.5 to 0.5
- admit_blocks: bfloat16 [16, 128, 128], P('tp'), may hold values from -0.5 to 0.5
- decay_logit: float32 [2048], P('tp'), may hold values from 3.5 to 9
- mix_out_gain: float32 [2048], P('tp'), may hold values from 0.1 to 1.9
- out_weight: bfloat16 [2048, 2048], P('tp', 'fs'), may hold values from -0.125 to 0.125
- ffn_gain: float32 [2048], replicated, may hold values from 0.1 to 1.9
- gate_weight: bfloat16 [2048, 2816], P('fs', 'tp'), may hold values from -0.125 to 0.125
- up_weight: bfloat16 [2048, 2816], P('fs', 'tp'), may hold values from -0.125 to 0.125
- gate_taps: float32 [3, 2816], P(None, 'tp'), may hold values from -3 to 3
- up_taps: float32 [3, 2816], P(None, 'tp'), may hold values from -3 to 3
- down_weight: bfloat16 [2816, 2048], P('tp', 'fs'), may hold values from -0.109375 to 0.109375
Outputs:
- stream_out: bfloat16 [64, 768, 2048], P(('rep', 'fs'), None, 'tp')
The draws below stay inside these ranges and needn't reach their ends.
All inputs are finite; a program needn't handle non-finite values.
Results may differ from the reference program's by a relative error of at most 0.018.
Values may be sent and summed in bfloat16 or wider, within the bound.
A program may use at most 128 MiB of HBM per device.

```python
import jax
import jax.numpy as jnp
from jax import lax

D = 2048
HD = 128
BLOCKS = 16
FF = 2816
LEN = 768
LRU = 2048
SEQS = 64
N_TP = 2


def steps_of(rng, dims, split, smallest, top_value):
    level = 1.0
    for axis_at, parts in split:
        heights = jax.random.uniform(jax.random.fold_in(jax.random.fold_in(rng, 6), axis_at), (parts,), jnp.float32, smallest / len(split), top_value / len(split))
        level = level * jnp.repeat(jnp.exp(heights), dims[axis_at] // parts).reshape((-1,) + (1,) * (len(dims) - 1 - axis_at))
    return level


def scatter_about(rng, dims, deviation, limit, cuts=(), held_as=jnp.bfloat16):
    level = steps_of(rng, dims, cuts, -0.22, 0.18) if cuts else 1.0
    array = jax.random.normal(rng, dims, jnp.float32) * deviation * level
    return jnp.minimum(jnp.maximum(array, -limit), limit).astype(held_as)


def setup_inputs(seed: int = 0) -> dict:
    streams_of = jax.random.split(jax.random.key(seed), 17)
    return {
        "stream_in": scatter_about(streams_of[0], (SEQS, LEN, D), 1.0, 6.0, ((0, 64), (2, 2))),
        "mix_gain": jnp.clip(1.0 + 0.18 * jax.random.normal(streams_of[1], (D,), jnp.float32), 0.1, 1.9),
        "lin_weight": scatter_about(streams_of[2], (D, LRU), D ** -0.5, 0.125, ((0, 32), (1, 2))),
        "branch_weight": scatter_about(streams_of[3], (D, LRU), D ** -0.5, 0.125, ((0, 32), (1, 2))),
        "lin_taps": scatter_about(streams_of[4], (4, LRU), 0.5, 3.0, ((1, 2),), jnp.float32),
        "rate_blocks": scatter_about(streams_of[5], (BLOCKS, HD, HD), HD ** -0.5, 0.5, ((0, 2),)),
        "admit_blocks": scatter_about(streams_of[6], (BLOCKS, HD, HD), HD ** -0.5, 0.5, ((0, 2),)),
        "decay_logit": jnp.clip(3.5 + 5.5 * jax.random.uniform(streams_of[7], (LRU,), jnp.float32) ** steps_of(streams_of[7], (LRU,), ((0, 2),), -0.2, 0.2), 3.5, 9.0),
        "mix_out_gain": jnp.clip(1.0 + 0.18 * jax.random.normal(streams_of[8], (LRU,), jnp.float32), 0.1, 1.9),
        "out_weight": scatter_about(streams_of[9], (LRU, D), LRU ** -0.5, 0.125, ((0, 2), (1, 32))),
        "ffn_gain": jnp.clip(1.0 + 0.18 * jax.random.normal(streams_of[10], (D,), jnp.float32), 0.1, 1.9),
        "gate_weight": scatter_about(streams_of[11], (D, FF), D ** -0.5, 0.125, ((0, 32), (1, 2))),
        "up_weight": scatter_about(streams_of[12], (D, FF), D ** -0.5, 0.125, ((0, 32), (1, 2))),
        "gate_taps": scatter_about(streams_of[13], (3, FF), 0.6, 3.0, ((1, 2),), jnp.float32),
        "up_taps": scatter_about(streams_of[14], (3, FF), 0.6, 3.0, ((1, 2),), jnp.float32),
        "down_weight": scatter_about(streams_of[15], (FF, D), FF ** -0.5, 0.109375, ((0, 2), (1, 32))),
    }


EPS = 1e-06
GATE_SCALE = 8.0

def norm_rows(values, scales):
    mean_sq = lax.optimization_barrier(jnp.mean(values * values, axis=-1, keepdims=True))
    return values * lax.rsqrt(mean_sq + EPS) * scales

def causal_filter(values, kernel):
    kernel_len = kernel.shape[0]
    seq_len = values.shape[0]
    padded = jnp.pad(values, ((kernel_len - 1, 0), (0, 0)))
    summed = padded[0:seq_len] * kernel[0]
    for offset in range(1, kernel_len):
        summed = summed + padded[offset:offset + seq_len] * kernel[offset]
    return summed

def chain_combine(earlier, later):
    return (earlier[0] * later[0], later[0] * earlier[1] + later[1])

def split_product(left, right):
    group = left.shape[1] // N_TP
    summed = jnp.zeros((left.shape[0], right.shape[1]), jnp.float32)
    for column_part in range(N_TP):
        partial_value = jnp.dot(left[:, column_part * group:(column_part + 1) * group], right[column_part * group:(column_part + 1) * group], preferred_element_type=jnp.float32)
        partial_value = lax.optimization_barrier(partial_value.astype(jnp.bfloat16))
        summed = summed + partial_value.astype(jnp.float32)
    return summed

def reference(stream_in, mix_gain, lin_weight, branch_weight, lin_taps, rate_blocks, admit_blocks, decay_logit, mix_out_gain, out_weight, ffn_gain, gate_weight, up_weight, gate_taps, up_taps, down_weight):

    def one_sequence(sequence):
        stream = sequence.astype(jnp.float32)
        normed = norm_rows(stream, mix_gain).astype(jnp.bfloat16)
        linear = jnp.dot(normed, lin_weight, preferred_element_type=jnp.float32).astype(jnp.bfloat16)
        branch = jnp.dot(normed, branch_weight, preferred_element_type=jnp.float32).astype(jnp.bfloat16)
        filtered = causal_filter(linear.astype(jnp.float32), lin_taps)
        blocks = filtered.astype(jnp.bfloat16).astype(jnp.float32).reshape(LEN, BLOCKS, HD)
        rate_gate = jax.nn.sigmoid(jnp.einsum('lbi,bij->lbj', blocks, rate_blocks.astype(jnp.float32)).reshape(LEN, BLOCKS * HD))
        admitted = jax.nn.sigmoid(jnp.einsum('lbi,bij->lbj', blocks, admit_blocks.astype(jnp.float32)).reshape(LEN, BLOCKS * HD))
        log_decay = -GATE_SCALE * rate_gate * jax.nn.softplus(-decay_logit)
        decay = jnp.exp(log_decay)
        driven = jnp.sqrt(-jnp.expm1(2.0 * log_decay)) * admitted * filtered
        _, states = lax.associative_scan(chain_combine, (decay, driven), axis=0)
        gated = (states * jax.nn.gelu(branch.astype(jnp.float32))).reshape(LEN, BLOCKS, HD)
        gated = gated * lax.rsqrt(lax.optimization_barrier(jnp.mean(gated * gated, axis=-1, keepdims=True)) + EPS)
        mixed = (gated.reshape(LEN, BLOCKS * HD) * mix_out_gain).astype(jnp.bfloat16)
        middle = (stream + split_product(mixed, out_weight)).astype(jnp.bfloat16)
        normed2 = norm_rows(middle.astype(jnp.float32), ffn_gain).astype(jnp.bfloat16)
        gate_pre = jnp.dot(normed2, gate_weight, preferred_element_type=jnp.float32).astype(jnp.bfloat16)
        up_pre = jnp.dot(normed2, up_weight, preferred_element_type=jnp.float32).astype(jnp.bfloat16)
        gate_conv = causal_filter(gate_pre.astype(jnp.float32), gate_taps)
        up_conv = causal_filter(up_pre.astype(jnp.float32), up_taps)
        hidden = (jax.nn.silu(gate_conv) * up_conv).astype(jnp.bfloat16)
        return (middle.astype(jnp.float32) + split_product(hidden, down_weight)).astype(jnp.bfloat16)
    return lax.map(one_sequence, stream_in)
```

```python
import functools

import jax
import jax.numpy as jnp
from jax import lax
from jax.experimental import pallas as pl
from jax.experimental.pallas import tpu as pltpu
from jax.sharding import PartitionSpec as P

EPS = 1e-06
GATE_SCALE = 8.0
MESH = pl.DeviceIdType.MESH
F32, BF16 = jnp.float32, jnp.bfloat16

GROUPS = ((16, (5, 5, 3, 3)), (8, (3, 2, 1, 2)), (22, (7, 7, 4, 4)), (11, (3, 4, 2, 2)))
FINE = (True, True, True, True)
LINK_RATE = 44.0e3
HOP_US = 2.2
SHARD_ROWS = 64


def region_slots(region):
    count = 2 if region[0] == "both" else 1
    for part in region[1:]:
        if not isinstance(part, int):
            count *= part[1] - part[0]
    return count


def tree_edges():
    edges = []
    for group, (_, split) in enumerate(GROUPS):
        first = 0
        for tree, width in enumerate(split):
            columns = (first * 128, width * 128)
            first += width
            fast, slow = ("x", "y") if tree % 2 == 0 else ("y", "x")

            def add(name, way, region, parents):
                z, f, s = region
                placed = (z, s, f) if fast == "x" else (z, f, s)
                edges.append(
                    dict(
                        key=(group, tree, name),
                        way=way,
                        region=placed,
                        columns=columns,
                        bytes=region_slots(region) * width * 128 * SHARD_ROWS * 2,
                        parents=[(group, tree, p) for p in parents],
                    )
                )

            flip = (group + tree) % 2
            one, two = ("+", "-") if flip == 0 else ("-", "+")
            if tree < 2:
                add("p+", fast + "+", ("own", 0, 0), [])
                add("p-", fast + "-", ("own", 0, 0), [])
                add("p2", fast + one, ("own", -1 if one == "+" else 1, 0), ["p" + one])
                for k, (r, par) in enumerate(((0, []), (-1, ["p+"]), (1, ["p-"]), (2, ["p2"]))):
                    add(f"q+{r}", slow + "+", ("own", r, 0), par)
                    add(f"q-{r}", slow + "-", ("own", r, 0), par)
                    a = "+" if (k + flip) % 2 else "-"
                    add(f"q2{r}", slow + a, ("own", r, -1 if a == "+" else 1), [f"q{a}{r}"])
                    za, zb = ("+", "-") if k % 2 else ("-", "+")
                    add(f"z0{r}", "z" + za, ("own", r, 0), par)
                    add(f"z1{r}", "z" + zb, ("own", r, -1), [f"q+{r}"])
                    add(f"z2{r}", "z" + za, ("own", r, 1), [f"q-{r}"])
                    add(f"z3{r}", "z" + zb, ("own", r, 2), [f"q2{r}"])
            else:
                add("z", "z" + ("+" if tree == 2 else "-"), ("own", 0, 0), [])
                for k, (z, par) in enumerate((("own", []), ("other", ["z"]))):
                    add(f"p+{z}", fast + "+", (z, 0, 0), par)
                    add(f"p-{z}", fast + "-", (z, 0, 0), par)
                    a = "+" if k else "-"
                    add(f"p2{z}", fast + a, (z, -1 if a == "+" else 1, 0), [f"p{a}{z}"])
                arrived = {
                    0: ["z"],
                    -1: ["p+own", "p+other"],
                    1: ["p-own", "p-other"],
                    2: ["p2own", "p2other"],
                }
                for k, r in enumerate((0, -1, 1, 2)):
                    add(f"q+{r}", slow + "+", ("both", r, 0), arrived[r])
                    add(f"q-{r}", slow + "-", ("both", r, 0), arrived[r])
                    a = "+" if (k + flip) % 2 else "-"
                    add(f"q2{r}", slow + a, ("both", r, -1 if a == "+" else 1), [f"q{a}{r}"])
    return edges


def planned(edges):
    index = {e["key"]: k for k, e in enumerate(edges)}
    free, landed, begun = {}, {}, {}
    waiting, order = list(range(len(edges))), []
    while waiting:
        best = None
        for k in waiting:
            e = edges[k]
            if any(index[p] not in landed for p in e["parents"]):
                continue
            ready = max([landed[index[p]] for p in e["parents"]], default=0.0)
            start = max(ready, free.get(e["way"], 0.0))
            rank = (start, e["key"][0], ready)
            if best is None or rank < best[0]:
                best = (rank, k, ready, start)
        _, k, ready, start = best
        free[edges[k]["way"]] = start + edges[k]["bytes"] / LINK_RATE
        landed[k] = free[edges[k]["way"]] + HOP_US
        begun[k] = (ready, start)
        waiting.remove(k)
        order.append(k)
    return index, order, landed, begun


class Gather:
    def __init__(self, edges, plan, buffers, send, recv):
        self.edges, self.buffers, self.send, self.recv = edges, buffers, send, recv
        self.index, self.order, self.landed, self.begun = plan
        self.seen, self.queue = set(), list(self.order)
        fs, rep = lax.axis_index("fs"), lax.axis_index("rep")
        x, y, half = lax.rem(fs, 4), lax.rem(lax.div(fs, 4), 4), lax.div(fs, 16)
        z = rep * 2 + half
        self.x = {r: (lax.rem(x + r + 4, 4) if r else x) for r in (-1, 0, 1, 2)}
        self.y = {r: (lax.rem(y + r + 4, 4) if r else y) for r in (-1, 0, 1, 2)}
        self.z = {"own": half, "other": 1 - half}
        self.device = {}
        for sign, d in (("+", 1), ("-", -1)):
            self.device["x" + sign] = {"fs": half * 16 + y * 4 + self.x[d]}
            self.device["y" + sign] = {"fs": half * 16 + self.y[d] * 4 + x}
            beyond = lax.rem(z + d + 4, 4)
            self.device["z" + sign] = {
                "rep": lax.div(beyond, 2),
                "fs": lax.rem(beyond, 2) * 16 + y * 4 + x,
            }

    def place(self, edge, arriving):
        z, y, x = edge["region"]
        axis, shift = edge["way"][0], (1 if edge["way"][1] == "+" else -1)

        def moved(part, name):
            if not isinstance(part, int):
                return part
            if arriving and axis == name:
                part -= shift
            return {-2: 2, 3: -1}.get(part, part)

        def cut(part, table):
            return table[part] if isinstance(part, int) else pl.ds(part[0], part[1] - part[0])

        if arriving and axis == "z":
            z = {"own": "other", "other": "own", "both": "both"}[z]
        at_z = pl.ds(0, 2) if z == "both" else self.z[z]
        start, width = edge["columns"]
        return self.buffers[edge["key"][0]].at[
            at_z, cut(moved(y, "y"), self.y), cut(moved(x, "x"), self.x), :, pl.ds(start, width)
        ]

    def copy(self, k, arriving):
        edge = self.edges[k]
        ref = self.place(edge, arriving)
        return pltpu.make_async_remote_copy(
            src_ref=ref,
            dst_ref=ref,
            send_sem=self.send.at[k],
            recv_sem=self.recv.at[k],
            device_id=self.device[edge["way"]],
            device_id_type=MESH,
        )

    def arrive(self, k):
        if k not in self.seen:
            self.seen.add(k)
            self.copy(k, True).wait_recv()

    def start(self, k):
        for p in self.edges[k]["parents"]:
            self.arrive(self.index[p])
        self.copy(k, False).start()

    def take(self, until):
        taken = []
        while self.queue and self.begun[self.queue[0]][1] <= until:
            taken.append(self.queue.pop(0))
        return taken

    def pump(self, until):
        for k in self.take(until):
            self.start(k)

    def group_done(self, group):
        members = [k for k in self.order if self.edges[k]["key"][0] == group]
        while any(k in self.queue for k in members) or any(
            self.index[p] in self.queue for k in members for p in self.edges[k]["parents"]
        ):
            self.start(self.queue.pop(0))
        for k in members:
            self.arrive(k)

    def finish(self):
        for k in self.order:
            self.copy(k, False).wait_send()


def at_step(step, count, gather, first, pace):
    for k in range(count):
        due = gather.take(first + pace * k)
        if due:

            @pl.when(step == k)
            def _(due=due):
                for one in due:
                    gather.start(one)


def shifted_down(values, amount, fill, row):
    return jnp.where(row >= amount, pltpu.roll(values, amount, 0), fill)


def scan_rows(decay, driven, row):
    rows = decay.shape[0]
    step = 1
    while step < rows:
        before_b = shifted_down(driven, step, 0.0, row)
        before_a = shifted_down(decay, step, 1.0, row)
        driven = decay * before_b + driven
        decay = decay * before_a
        step *= 2
    return decay, driven


LEN = 768
BLOCK = 128
ROWS = 256
NORM_ROWS = 16


def kernel(edges, plan, *refs):
    (x, gain, lin, branch, taps, rate, admit, logit, mix_gain, out_w, ffn_gain, gate, up, gate_taps, up_taps, down) = refs[:16]
    result = refs[16]
    (b0, b1, b2, b3, full, normed, mixed, sent, got, hidden, dsent, dgot, pad_a, pad_b, send, recv, load, xsem, osend, orecv, dsend, drecv) = refs[17:]
    tp = lax.axis_index("tp")
    gather = Gather(edges, plan, (b0, b1, b2, b3), send, recv)
    partner = {"tp": 1 - tp}
    zl, y0, x0 = gather.z["own"], gather.y[0], gather.x[0]

    loads = [pltpu.make_async_copy(x, full.at[tp], load.at[0])]
    pieces = [(out_w, b1, 0, 0, 1024), (down, b3, 0, 0, 1408)]
    for k in range(8):
        pieces += [(lin, b0, k * 128, k * 256, 128), (branch, b0, k * 128, k * 256 + 128, 128)]
    for k in range(11):
        pieces += [(gate, b2, k * 128, k * 256, 128), (up, b2, k * 128, k * 256 + 128, 128)]
    for k, (source, target, at, to, width) in enumerate(pieces):
        loads.append(
            pltpu.make_async_copy(
                source.at[:, pl.ds(at, width)], target.at[zl, y0, x0, :, pl.ds(to, width)], load.at[k + 1]
            )
        )
    for one in loads:
        one.start()
    barrier = pltpu.get_barrier_semaphore()
    for device in [*gather.device.values(), partner]:
        pl.semaphore_signal(barrier, inc=1, device_id=device, device_id_type=MESH)
    pl.semaphore_wait(barrier, 7)
    x_copy = pltpu.make_async_remote_copy(
        src_ref=x, dst_ref=full.at[tp], send_sem=xsem.at[0], recv_sem=xsem.at[1], device_id=partner, device_id_type=MESH
    )
    x_copy.start()
    for one in loads:
        one.wait()
    gather.pump(LEAD_US)
    x_copy.wait_send()
    pltpu.make_async_remote_copy(
        src_ref=x, dst_ref=full.at[1 - tp], send_sem=xsem.at[0], recv_sem=xsem.at[1], device_id=partner, device_id_type=MESH
    ).wait_recv()

    def norm(chunk, scales, with_sums):
        rows = pl.ds(pl.multiple_of(chunk * NORM_ROWS, NORM_ROWS), NORM_ROWS)
        halves = []
        for h in range(2):
            part = full[h, rows, :].astype(F32)
            if with_sums:
                extra = [
                    sent[h, q, rows, :].astype(F32) + got[h, q, rows, :].astype(F32) for q in range(4)
                ]
                rounded = (part + jnp.concatenate(extra, axis=1)).astype(BF16)
                full[h, rows, :] = rounded
                part = rounded.astype(F32)
            halves.append(part)
        total = sum(jnp.sum(part * part, axis=-1, keepdims=True) for part in halves)
        factor = lax.rsqrt(total * (1.0 / 2048.0) + EPS)
        for h in range(2):
            normed[h, rows, :] = (halves[h] * factor * scales[h : h + 1, :]).astype(BF16)

    @pl.loop(0, LEN // NORM_ROWS)
    def _(chunk):
        norm(chunk, gain, False)

    pad_a[0:8, :] = jnp.zeros((8, BLOCK), F32)
    pad_b[0:8, :] = jnp.zeros((8, BLOCK), F32)
    row = lax.broadcasted_iota(jnp.int32, (ROWS, BLOCK), 0)
    gather.group_done(0)

    def both(buffer, step):
        columns = pl.ds(pl.multiple_of(step * 256, 256), 256)
        total = None
        for h in range(2):
            weights = buffer[h, :, :, :, columns].reshape(1024, 256)
            part = jnp.dot(normed[h], weights, preferred_element_type=F32)
            total = part if total is None else total + part
        return total.astype(BF16).astype(F32)

    @pl.loop(0, 8)
    def _(step):
        at_step(step, 8, gather, *MIX_PACE)
        lanes = pl.ds(pl.multiple_of(step * BLOCK, BLOCK), BLOCK)
        values = both(b0, step)
        pad_a[8 : 8 + LEN, :] = values[:, :BLOCK]
        pad_b[8 : 8 + LEN, :] = values[:, BLOCK:]
        tap = taps[:, lanes]
        base = -GATE_SCALE * jax.nn.softplus(-logit[:, lanes])
        scale = mix_gain[:, lanes]
        carry = jnp.zeros((1, BLOCK), F32)
        for c in range(LEN // ROWS):
            at = c * ROWS
            filtered = sum(pad_a[5 + j + at : 5 + j + at + ROWS, :] * tap[j : j + 1, :] for j in range(4))
            rounded = filtered.astype(BF16)
            rate_gate = jax.nn.sigmoid(jnp.dot(rounded, rate[step], preferred_element_type=F32))
            admitted = jax.nn.sigmoid(jnp.dot(rounded, admit[step], preferred_element_type=F32))
            log_decay = rate_gate * base
            decay = jnp.exp(log_decay)
            rest = -jnp.tanh(log_decay) * (1.0 + decay * decay)
            driven = jnp.sqrt(rest) * admitted * filtered
            product, states = scan_rows(decay, driven, row)
            states = states + product * carry
            carry = states[ROWS - 1 : ROWS, :]
            gated = states * jax.nn.gelu(pad_b[8 + at : 8 + at + ROWS, :], approximate=True)
            mean = jnp.mean(gated * gated, axis=-1, keepdims=True)
            mixed[at : at + ROWS, lanes] = (gated * lax.rsqrt(mean + EPS) * scale).astype(BF16)

    gather.group_done(1)

    def out_copy(j):
        h, q = lax.rem(1 - tp + lax.div(j, 4), 2), lax.rem(j, 4)
        return pltpu.make_async_remote_copy(
            src_ref=sent.at[h, q], dst_ref=got.at[h, q], send_sem=osend.at[j], recv_sem=orecv.at[j],
            device_id=partner, device_id_type=MESH,
        )

    def arriving_copy(j):
        h, q = lax.rem(tp + lax.div(j, 4), 2), lax.rem(j, 4)
        return pltpu.make_async_remote_copy(
            src_ref=sent.at[h, q], dst_ref=got.at[h, q], send_sem=osend.at[j], recv_sem=orecv.at[j],
            device_id=partner, device_id_type=MESH,
        )

    @pl.loop(0, 8)
    def _(j):
        at_step(j, 8, gather, *OUT_PACE)
        h, q = lax.rem(1 - tp + lax.div(j, 4), 2), lax.rem(j, 4)
        weights = b1[h, q].reshape(256, 1024)
        part = lax.dot_general(mixed[...], weights, (((1,), (1,)), ((), ())), preferred_element_type=F32)
        sent[h, q] = part.astype(BF16)

        @pl.when(j > 0)
        def _():
            out_copy(j - 1).start()

    out_copy(7).start()
    gather.pump(NORM2_US)
    for j in range(8):
        arriving_copy(j).wait_recv()

    @pl.loop(0, LEN // NORM_ROWS)
    def _(chunk):
        norm(chunk, ffn_gain, True)

    gather.group_done(2)

    @pl.loop(0, 11)
    def _(step):
        at_step(step, 11, gather, *FFN_PACE)
        lanes = pl.ds(pl.multiple_of(step * BLOCK, BLOCK), BLOCK)
        values = both(b2, step)
        pad_a[8 : 8 + LEN, :] = values[:, :BLOCK]
        pad_b[8 : 8 + LEN, :] = values[:, BLOCK:]
        tap_g, tap_u = gate_taps[:, lanes], up_taps[:, lanes]
        for c in range(LEN // ROWS):
            at = c * ROWS
            conv_g = sum(pad_a[6 + j + at : 6 + j + at + ROWS, :] * tap_g[j : j + 1, :] for j in range(3))
            conv_u = sum(pad_b[6 + j + at : 6 + j + at + ROWS, :] * tap_u[j : j + 1, :] for j in range(3))
            hidden[at : at + ROWS, lanes] = (jax.nn.silu(conv_g) * conv_u).astype(BF16)

    gather.group_done(3)

    def down_copy(q):
        return pltpu.make_async_remote_copy(
            src_ref=dsent.at[q], dst_ref=dgot.at[q], send_sem=dsend.at[q], recv_sem=drecv.at[q],
            device_id=partner, device_id_type=MESH,
        )

    def down_part(h, q):
        weights = b3[h, q].reshape(256, 1408)
        part = lax.dot_general(hidden[...], weights, (((1,), (1,)), ((), ())), preferred_element_type=F32)
        return part.astype(BF16)

    @pl.loop(0, 8)
    def _(j):
        h, q = lax.rem(1 - tp + lax.div(j, 4), 2), lax.rem(j, 4)
        part = down_part(h, q)

        @pl.when(j < 4)
        def _():
            dsent[q] = part

        @pl.when((j > 0) & (j < 5))
        def _():
            down_copy(j - 1).start()

        @pl.when(j >= 4)
        def _():
            down_copy(q).wait_recv()
            lanes = pl.ds(pl.multiple_of(q * 256, 256), 256)
            total = part.astype(F32) + dgot[q].astype(F32)
            result[:, lanes] = (full[tp, :, lanes].astype(F32) + total).astype(BF16)

    for j in range(8):
        out_copy(j).wait_send()
    for q in range(4):
        down_copy(q).wait_send()
    gather.finish()


LEAD_US = 1e9
MIX_PACE = (1e9, 0.0)
OUT_PACE = (1e9, 0.0)
NORM2_US = 1e9
FFN_PACE = (1e9, 0.0)


def local(
    stream_in, mix_gain, lin_weight, branch_weight, lin_taps, rate_blocks, admit_blocks, decay_logit, mix_out_gain,
    out_weight, ffn_gain, gate_weight, up_weight, gate_taps, up_taps, down_weight,
):
    edges = tree_edges()
    plan = planned(edges)
    count = len(edges)
    any_space, vmem = pl.BlockSpec(memory_space=pl.ANY), pl.BlockSpec(memory_space=pltpu.VMEM)
    operands = [
        (stream_in[0], any_space),
        (mix_gain.reshape(2, 1024), vmem),
        (lin_weight, any_space),
        (branch_weight, any_space),
        (lin_taps, vmem),
        (rate_blocks, vmem),
        (admit_blocks, vmem),
        (decay_logit.reshape(1, 1024), vmem),
        (mix_out_gain.reshape(1, 1024), vmem),
        (out_weight.T, any_space),
        (ffn_gain.reshape(2, 1024), vmem),
        (gate_weight, any_space),
        (up_weight, any_space),
        (gate_taps, vmem),
        (up_taps, vmem),
        (down_weight.T, any_space),
    ]
    dma = pltpu.SemaphoreType.DMA
    result = pl.pallas_call(
        functools.partial(kernel, edges, plan),
        out_shape=jax.ShapeDtypeStruct((LEN, 1024), BF16),
        in_specs=[spec for _, spec in operands],
        out_specs=vmem,
        scratch_shapes=[
            pltpu.VMEM((2, 4, 4, SHARD_ROWS, 2048), BF16),
            pltpu.VMEM((2, 4, 4, SHARD_ROWS, 1024), BF16),
            pltpu.VMEM((2, 4, 4, SHARD_ROWS, 2816), BF16),
            pltpu.VMEM((2, 4, 4, SHARD_ROWS, 1408), BF16),
            pltpu.VMEM((2, LEN, 1024), BF16),
            pltpu.VMEM((2, LEN, 1024), BF16),
            pltpu.VMEM((LEN, 1024), BF16),
            pltpu.VMEM((2, 4, LEN, 256), BF16),
            pltpu.VMEM((2, 4, LEN, 256), BF16),
            pltpu.VMEM((LEN, 1408), BF16),
            pltpu.VMEM((4, LEN, 256), BF16),
            pltpu.VMEM((4, LEN, 256), BF16),
            pltpu.VMEM((LEN + 8, BLOCK), F32),
            pltpu.VMEM((LEN + 8, BLOCK), F32),
            dma((count,)), dma((count,)), dma((41,)), dma((2,)), dma((8,)), dma((8,)), dma((4,)), dma((4,)),
        ],
        compiler_params=pltpu.CompilerParams(
            collective_id=0, has_side_effects=True, vmem_limit_bytes=63 * 1024 * 1024
        ),
    )(*[array for array, _ in operands])
    return result[None]


def solution(mesh):
    placed = (
        P(("rep", "fs"), None, "tp"), P(), P("fs", "tp"), P("fs", "tp"), P(None, "tp"), P("tp", None, None),
        P("tp", None, None), P("tp"), P("tp"), P("tp", "fs"), P(), P("fs", "tp"), P("fs", "tp"), P(None, "tp"),
        P(None, "tp"), P("tp", "fs"),
    )
    return jax.shard_map(
        local, mesh=mesh, in_specs=placed, out_specs=P(("rep", "fs"), None, "tp"), check_vma=False
    )
```

```python
import functools

import jax
import jax.numpy as jnp
from jax import lax
from jax.experimental import pallas as pl
from jax.experimental.pallas import tpu as pltpu
from jax.sharding import PartitionSpec as P

EPS = 1e-06
GATE_SCALE = 8.0
MESH = pl.DeviceIdType.MESH
F32, BF16 = jnp.float32, jnp.bfloat16

GROUPS = (
    (0, 0, (5, 5, 3, 3)),
    (1, 0, (3, 2, 1, 2)),
    (2, 0, (7, 7, 4, 4)),
    (3, 0, (3, 4, 2, 2)),
)
LINK_RATE = 48000.0
HOP_US = 3.0
EARLY_US = 100.0
GATE_UP, DOWN = (2, 2), 3
ROW_STEPS = (0, 1, -1, 2)
ROW_ORDER = tuple((half, step) for half in ("own", "other") for step in ROW_STEPS)
SHARD_ROWS = 64


def region_slots(region):
    count = 2 if region[0] == "both" else 1
    for part in region[1:]:
        if not isinstance(part, int):
            count *= part[1] - part[0]
    return count


def tree_edges():
    edges = []
    for group, (buffer, first, split) in enumerate(GROUPS):
        for tree, width in enumerate(split):
            columns = (first * 128, width * 128)
            first += width
            fast, slow = ("x", "y") if tree % 2 == 0 else ("y", "x")

            def add(name, way, region, parents):
                z, f, s = region
                placed = (z, s, f) if fast == "x" else (z, f, s)
                edges.append(
                    dict(
                        key=(group, tree, name),
                        way=way,
                        buffer=buffer,
                        region=placed,
                        columns=columns,
                        bytes=region_slots(region) * width * 128 * SHARD_ROWS * 2,
                        parents=[(group, tree, p) for p in parents],
                    )
                )

            flip = (group + tree) % 2
            one, two = ("+", "-") if flip == 0 else ("-", "+")
            if tree < 2:
                add("p+", fast + "+", ("own", 0, 0), [])
                add("p-", fast + "-", ("own", 0, 0), [])
                add("p2", fast + one, ("own", -1 if one == "+" else 1, 0), ["p" + one])
                for k, (r, par) in enumerate(((0, []), (-1, ["p+"]), (1, ["p-"]), (2, ["p2"]))):
                    add(f"q+{r}", slow + "+", ("own", r, 0), par)
                    add(f"q-{r}", slow + "-", ("own", r, 0), par)
                    a = "+" if (k + flip) % 2 else "-"
                    add(f"q2{r}", slow + a, ("own", r, -1 if a == "+" else 1), [f"q{a}{r}"])
                    za, zb = ("+", "-") if k % 2 else ("-", "+")
                    add(f"z0{r}", "z" + za, ("own", r, 0), par)
                    add(f"z1{r}", "z" + zb, ("own", r, -1), [f"q+{r}"])
                    add(f"z2{r}", "z" + za, ("own", r, 1), [f"q-{r}"])
                    add(f"z3{r}", "z" + zb, ("own", r, 2), [f"q2{r}"])
            else:
                add("z", "z" + ("+" if tree == 2 else "-"), ("own", 0, 0), [])
                for k, (z, par) in enumerate((("own", []), ("other", ["z"]))):
                    add(f"p+{z}", fast + "+", (z, 0, 0), par)
                    add(f"p-{z}", fast + "-", (z, 0, 0), par)
                    a = "+" if k else "-"
                    add(f"p2{z}", fast + a, (z, -1 if a == "+" else 1, 0), [f"p{a}{z}"])
                arrived = {
                    0: ["z"],
                    -1: ["p+own", "p+other"],
                    1: ["p-own", "p-other"],
                    2: ["p2own", "p2other"],
                }
                for k, r in enumerate((0, -1, 1, 2)):
                    add(f"q+{r}", slow + "+", ("both", r, 0), arrived[r])
                    add(f"q-{r}", slow + "-", ("both", r, 0), arrived[r])
                    a = "+" if (k + flip) % 2 else "-"
                    add(f"q2{r}", slow + a, ("both", r, -1 if a == "+" else 1), [f"q{a}{r}"])
    return edges


def landing(edge):
    z, y, x = edge["region"]
    shift = 1 if edge["way"][1] == "+" else -1
    if edge["way"][0] == "z":
        return {"own": "other", "other": "own", "both": "both"}[z], y, x
    wrap = {-2: 2, 3: -1}
    if edge["way"][0] == "y":
        return z, wrap.get(y - shift, y - shift), x
    return z, y, wrap.get(x - shift, x - shift)


def in_row(edge, row):
    z, y, _ = landing(edge)
    return z in (row[0], "both") and y == row[1]


def planned(edges):
    index = {e["key"]: k for k, e in enumerate(edges)}
    free, landed, begun = {}, {}, {}
    waiting, order = list(range(len(edges))), []
    while waiting:
        best = None
        for k in waiting:
            e = edges[k]
            if any(index[p] not in landed for p in e["parents"]):
                continue
            ready = max([landed[index[p]] for p in e["parents"]], default=0.0)
            start = max(ready, free.get(e["way"], 0.0))
            if best is None or (start, e["key"][0], ready) < best[0]:
                best = ((start, e["key"][0], ready), k, ready, start)
        _, k, ready, start = best
        free[edges[k]["way"]] = start + edges[k]["bytes"] / LINK_RATE
        landed[k] = free[edges[k]["way"]] + HOP_US
        begun[k] = (ready, start)
        waiting.remove(k)
        order.append(k)
    last, due = {}, {}
    for k in order:
        due[k] = max(begun[k][0], begun[k][1] - EARLY_US, last.get(edges[k]["way"], 0.0))
        last[edges[k]["way"]] = due[k]
    order.sort(key=lambda k: (due[k], begun[k][1]))
    return index, order, landed, due


class Gather:
    def __init__(self, edges, plan, buffers, send, recv):
        self.edges, self.buffers, self.send, self.recv = edges, buffers, send, recv
        self.index, self.order, self.landed, self.due = plan
        self.seen, self.queue = set(), list(self.order)
        fs, rep = lax.axis_index("fs"), lax.axis_index("rep")
        x, y, half = lax.rem(fs, 4), lax.rem(lax.div(fs, 4), 4), lax.div(fs, 16)
        z = rep * 2 + half
        self.x = {r: (lax.rem(x + r + 4, 4) if r else x) for r in (-1, 0, 1, 2)}
        self.y = {r: (lax.rem(y + r + 4, 4) if r else y) for r in (-1, 0, 1, 2)}
        self.z = {"own": half, "other": 1 - half}
        self.device = {}
        for sign, d in (("+", 1), ("-", -1)):
            self.device["x" + sign] = {"fs": half * 16 + y * 4 + self.x[d]}
            self.device["y" + sign] = {"fs": half * 16 + self.y[d] * 4 + x}
            beyond = lax.rem(z + d + 4, 4)
            self.device["z" + sign] = {
                "rep": lax.div(beyond, 2),
                "fs": lax.rem(beyond, 2) * 16 + y * 4 + x,
            }

    def place(self, edge, arriving):
        z, y, x = landing(edge) if arriving else edge["region"]
        at_z = pl.ds(0, 2) if z == "both" else self.z[z]
        start, width = edge["columns"]
        return self.buffers[edge["buffer"]].at[
            at_z, self.y[y], self.x[x], :, pl.ds(start, width)
        ]

    def copy(self, k, arriving):
        edge = self.edges[k]
        ref = self.place(edge, arriving)
        return pltpu.make_async_remote_copy(
            src_ref=ref,
            dst_ref=ref,
            send_sem=self.send.at[k],
            recv_sem=self.recv.at[k],
            device_id=self.device[edge["way"]],
            device_id_type=MESH,
        )

    def arrivals(self, ks):
        found = [k for k in ks if k not in self.seen]
        self.seen.update(found)
        return [(True, k) for k in found]

    def begin(self, k):
        return self.arrivals([self.index[p] for p in self.edges[k]["parents"]]) + [(False, k)]

    def due_by(self, until):
        steps = []
        while self.queue and self.due[self.queue[0]] <= until:
            steps += self.begin(self.queue.pop(0))
        return steps

    def members(self, group):
        return [k for k in self.order if self.edges[k]["key"][0] == group]

    def run(self, steps):
        for arriving, k in steps:
            if arriving:
                self.copy(k, True).wait_recv()
            else:
                self.copy(k, False).start()

    def pump(self, until):
        self.run(self.due_by(until))

    def until_done(self, group, row=None):
        members = self.members(group)
        if row is not None:
            members = [k for k in members if in_row(self.edges[k], row)]
        steps = self.due_by(max([self.landed[k] for k in members], default=0.0) - HOP_US)
        while any(k in self.queue for k in members) or any(
            self.index[p] in self.queue for k in members for p in self.edges[k]["parents"]
        ):
            steps += self.begin(self.queue.pop(0))
        return steps + self.arrivals(members)

    def group_done(self, group):
        self.run(self.until_done(group))

    def group_time(self, group):
        return max([self.landed[k] for k in self.members(group)], default=0.0)

    def timetable(self, count, first, pace, subs=1):
        return [
            [self.due_by(first + pace * (k + j / subs)) for j in range(subs)] for k in range(count)
        ]

    def sent(self, group):
        for k in self.members(group):
            self.copy(k, False).wait_send()


def at_step(step, table, gather, sub=0):
    for k, steps in enumerate(table):
        if steps[sub]:

            @pl.when(step == k)
            def _(steps=steps[sub]):
                gather.run(steps)


def shifted_down(values, amount, fill, row):
    return jnp.where(row >= amount, pltpu.roll(values, amount, 0), fill)


def scan_rows(decay, driven, row):
    rows = decay.shape[0]
    step = 1
    while step < rows:
        before_b = shifted_down(driven, step, 0.0, row)
        before_a = shifted_down(decay, step, 1.0, row)
        driven = decay * before_b + driven
        decay = decay * before_a
        step *= 2
    return decay, driven


LEN = 768
BLOCK = 128
ROWS = 256
NORM_ROWS = 16


def kernel(edges, plan, *refs):
    (x, gain, lin, branch, taps, rate, admit, logit, mix_gain, out_w, ffn_gain, gate, up, gate_taps, up_taps, down) = refs[:16]
    result = refs[16]
    small = (gain, taps, rate, admit, logit, mix_gain, ffn_gain, gate_taps, up_taps)
    held = refs[17 : 17 + len(small)]
    (b0, b1, b2, b3, full, normed, mixed, sent, got, hidden, dgot, final, pad_a, pad_b) = refs[26:40]
    (send, recv, load, ssem, xsem, osend, orecv, dsend, drecv, fsem) = refs[40:]
    tp = lax.axis_index("tp")
    gather = Gather(edges, plan, (b0, b1, b2, b3), send, recv)
    partner = {"tp": 1 - tp}
    zl, y0, x0 = gather.z["own"], gather.y[0], gather.x[0]

    x_load = pltpu.make_async_copy(x, full.at[tp], load.at[0])
    small_loads = [pltpu.make_async_copy(a, b, ssem.at[k]) for k, (a, b) in enumerate(zip(small, held))]
    (gain, taps, rate, admit, logit, mix_gain, ffn_gain, gate_taps, up_taps) = held
    loads = []
    pieces = [(out_w, b1, 0, 0, 1024), (down, b3, 0, 0, 1408)]
    for k in range(8):
        pieces += [(lin, b0, k * 128, k * 256, 128), (branch, b0, k * 128, k * 256 + 128, 128)]
    for k in range(11):
        pieces += [(gate, b2, k * 128, k * 256, 128), (up, b2, k * 128, k * 256 + 128, 128)]
    for k, (source, target, at, to, width) in enumerate(pieces):
        loads.append(
            pltpu.make_async_copy(
                source.at[:, pl.ds(at, width)], target.at[zl, y0, x0, :, pl.ds(to, width)], load.at[k + 1]
            )
        )
    for one in loads:
        one.start()
    barrier = pltpu.get_barrier_semaphore()
    for device in [*gather.device.values(), partner]:
        pl.semaphore_signal(barrier, inc=1, device_id=device, device_id_type=MESH)
    pl.semaphore_wait(barrier, 7)
    x_copy = pltpu.make_async_remote_copy(
        src_ref=x, dst_ref=full.at[tp], send_sem=xsem.at[0], recv_sem=xsem.at[1], device_id=partner, device_id_type=MESH
    )
    for one in loads:
        one.wait()
    gather.pump(0.0)
    x_copy.start()
    x_load.start()
    for one in small_loads:
        one.start()
    gather.pump(LEAD_US)
    x_load.wait()
    for one in small_loads:
        one.wait()
    x_copy.wait_send()
    pltpu.make_async_remote_copy(
        src_ref=x, dst_ref=full.at[1 - tp], send_sem=xsem.at[0], recv_sem=xsem.at[1], device_id=partner, device_id_type=MESH
    ).wait_recv()

    def norm(chunk, scales, with_sums):
        rows = pl.ds(pl.multiple_of(chunk * NORM_ROWS, NORM_ROWS), NORM_ROWS)
        halves = []
        for h in range(2):
            part = full[h, rows, :].astype(F32)
            if with_sums:
                extra = [
                    sent[h, q, rows, :].astype(F32) + got[h, q, rows, :].astype(F32) for q in range(4)
                ]
                rounded = (part + jnp.concatenate(extra, axis=1)).astype(BF16)
                full[h, rows, :] = rounded
                part = rounded.astype(F32)
            halves.append(part)
        total = sum(jnp.sum(part * part, axis=-1, keepdims=True) for part in halves)
        factor = lax.rsqrt(total * (1.0 / 2048.0) + EPS)
        for h in range(2):
            normed[h, rows, :] = (halves[h] * factor * scales[:, h * 1024 : h * 1024 + 1024]).astype(BF16)

    table = gather.timetable(LEN // NORM_ROWS // 6, *NORM_PACE)

    @pl.loop(0, LEN // NORM_ROWS // 6)
    def _(part):
        at_step(part, table, gather)

        @pl.loop(0, 6)
        def _(chunk):
            norm(part * 6 + chunk, gain, False)

    pad_a[0:8, :] = jnp.zeros((8, BLOCK), F32)
    pad_b[0:8, :] = jnp.zeros((8, BLOCK), F32)
    row = lax.broadcasted_iota(jnp.int32, (ROWS, BLOCK), 0)
    gather.group_done(0)
    start = gather.group_time(0)

    def both(buffer, step):
        columns = pl.ds(pl.multiple_of(step * 256, 256), 256)
        total = None
        for h in range(2):
            weights = buffer[h, :, :, :, columns].reshape(1024, 256)
            part = jnp.dot(normed[h], weights, preferred_element_type=F32)
            total = part if total is None else total + part
        return total.astype(BF16).astype(F32)

    table1 = gather.timetable(8, start + MIX_PACE[0], MIX_PACE[1], 4)

    @pl.loop(0, 8)
    def _(step):
        at_step(step, table1, gather, 0)
        lanes = pl.ds(pl.multiple_of(step * BLOCK, BLOCK), BLOCK)
        values = both(b0, step)
        pad_a[8 : 8 + LEN, :] = values[:, :BLOCK]
        pad_b[8 : 8 + LEN, :] = values[:, BLOCK:]
        tap = taps[:, lanes]
        base = -GATE_SCALE * jax.nn.softplus(-logit[:, lanes])
        scale = mix_gain[:, lanes]
        carry = jnp.zeros((1, BLOCK), F32)
        for c in range(LEN // ROWS):
            at_step(step, table1, gather, c + 1)
            at = c * ROWS
            filtered = sum(pad_a[5 + j + at : 5 + j + at + ROWS, :] * tap[j : j + 1, :] for j in range(4))
            rounded = filtered.astype(BF16)
            rate_gate = jax.nn.sigmoid(jnp.dot(rounded, rate[step], preferred_element_type=F32))
            admitted = jax.nn.sigmoid(jnp.dot(rounded, admit[step], preferred_element_type=F32))
            log_decay = rate_gate * base
            decay = jnp.exp(log_decay)
            rest = -jnp.tanh(log_decay) * (1.0 + decay * decay)
            driven = jnp.sqrt(rest) * admitted * filtered
            product, states = scan_rows(decay, driven, row)
            states = states + product * carry
            carry = states[ROWS - 1 : ROWS, :]
            gated = states * jax.nn.gelu(pad_b[8 + at : 8 + at + ROWS, :], approximate=True)
            mean = jnp.mean(gated * gated, axis=-1, keepdims=True)
            mixed[at : at + ROWS, lanes] = (gated * lax.rsqrt(mean + EPS) * scale).astype(BF16)

    gather.group_done(1)

    def out_copy(j):
        h, q = lax.rem(1 - tp + lax.div(j, 4), 2), lax.rem(j, 4)
        return pltpu.make_async_remote_copy(
            src_ref=sent.at[h, q], dst_ref=got.at[h, q], send_sem=osend.at[j], recv_sem=orecv.at[j],
            device_id=partner, device_id_type=MESH,
        )

    def arriving_copy(j):
        h, q = lax.rem(tp + lax.div(j, 4), 2), lax.rem(j, 4)
        return pltpu.make_async_remote_copy(
            src_ref=sent.at[h, q], dst_ref=got.at[h, q], send_sem=osend.at[j], recv_sem=orecv.at[j],
            device_id=partner, device_id_type=MESH,
        )

    table2 = gather.timetable(8, start + OUT_PACE[0], OUT_PACE[1])

    @pl.loop(0, 8)
    def _(j):
        at_step(j, table2, gather)
        h, q = lax.rem(1 - tp + lax.div(j, 4), 2), lax.rem(j, 4)
        weights = b1[h, q].reshape(256, 1024)
        part = lax.dot_general(mixed[...], weights, (((1,), (1,)), ((), ())), preferred_element_type=F32)
        sent[h, q] = part.astype(BF16)

        @pl.when(j > 0)
        def _():
            out_copy(j - 1).start()

    out_copy(7).start()
    gather.pump(start + NORM2_US)
    for j in range(8):
        arriving_copy(j).wait_recv()

    table3 = gather.timetable(LEN // NORM_ROWS // 6, start + NORM2_US, NORM_PACE[1])

    @pl.loop(0, LEN // NORM_ROWS // 6)
    def _(part):
        at_step(part, table3, gather)

        @pl.loop(0, 6)
        def _(chunk):
            norm(part * 6 + chunk, ffn_gain, True)

    for j in range(8):
        out_copy(j).wait_send()
    gather.sent(0)
    gather.group_done(GATE_UP[0])
    ready = gather.group_time(GATE_UP[0])
    table4 = gather.timetable(6, ready + FFN_PACE[0], FFN_PACE[1], 2)
    middle = gather.until_done(GATE_UP[1])
    later = max(ready + 6 * FFN_PACE[1], gather.group_time(GATE_UP[1])) + FFN_PACE[0]
    table5 = gather.timetable(5, later, FFN_PACE[1], 2)
    table4 = table4 + [[middle + table5[0][0], table5[0][1]]] + table5[1:]

    @pl.loop(0, 11)
    def _(step):
        at_step(step, table4, gather, 0)
        lanes = pl.ds(pl.multiple_of(step * BLOCK, BLOCK), BLOCK)
        values = both(b2, step)
        pad_a[8 : 8 + LEN, :] = values[:, :BLOCK]
        pad_b[8 : 8 + LEN, :] = values[:, BLOCK:]
        at_step(step, table4, gather, 1)
        tap_g, tap_u = gate_taps[:, lanes], up_taps[:, lanes]
        for c in range(LEN // ROWS):
            at = c * ROWS
            conv_g = sum(pad_a[6 + j + at : 6 + j + at + ROWS, :] * tap_g[j : j + 1, :] for j in range(3))
            conv_u = sum(pad_b[6 + j + at : 6 + j + at + ROWS, :] * tap_u[j : j + 1, :] for j in range(3))
            hidden[at : at + ROWS, lanes] = (jax.nn.silu(conv_g) * conv_u).astype(BF16)

    tables = [[gather.until_done(DOWN, row)] for row in ROW_ORDER]

    def row_of(j):
        k = lax.rem(j, 4)
        step = jnp.where(k == 2, 3, jnp.where(k == 3, 2, k))
        return lax.rem(zl + lax.div(j, 4), 2), lax.rem(y0 + step, 4)

    def down_copy(q):
        return pltpu.make_async_remote_copy(
            src_ref=sent.at[0, q], dst_ref=dgot.at[q], send_sem=dsend.at[q], recv_sem=drecv.at[q],
            device_id=partner, device_id_type=MESH,
        )

    def final_copy(q):
        lanes = pl.ds(pl.multiple_of(q * 256, 256), 256)
        return pltpu.make_async_copy(final.at[:, lanes], result.at[:, lanes], fsem.at[q])

    def complete(j):
        _, q = row_of(j)
        down_copy(q).wait_recv()
        lanes = pl.ds(pl.multiple_of(q * 256, 256), 256)
        total = sent[1, q].astype(F32) + dgot[q].astype(F32)
        final[:, lanes] = (full[tp, :, lanes].astype(F32) + total).astype(BF16)
        final_copy(q).start()

    def pass_on(j):
        h, q = row_of(j)

        @pl.when(h != tp)
        def _():
            down_copy(q).start()

    @pl.loop(0, 8)
    def _(j):
        at_step(j, tables, gather)
        h, q = row_of(j)
        weights = b3[h, q].reshape(256, 1408)
        part = lax.dot_general(hidden[...], weights, (((1,), (1,)), ((), ())), preferred_element_type=F32)
        sent[jnp.where(h == tp, 1, 0), q] = part.astype(BF16)

        @pl.when(j > 0)
        def _():
            pass_on(j - 1)

        @pl.when(j >= 6)
        def _():
            complete(j - 6)

    pass_on(7)
    gather.pump(1e9)
    for group in range(1, DOWN):
        gather.sent(group)
    complete(2)
    complete(3)
    gather.sent(DOWN)
    for q in range(4):
        down_copy(q).wait_send()
        final_copy(q).wait()


LEAD_US = 3.0
NORM_PACE = (3.0, 0.9)
MIX_PACE = (4.0, 3.0)
OUT_PACE = (28.0, 0.8)
NORM2_US = 37.0
FFN_PACE = (4.0, 1.6)


def local(
    stream_in, mix_gain, lin_weight, branch_weight, lin_taps, rate_blocks, admit_blocks, decay_logit, mix_out_gain,
    out_weight, ffn_gain, gate_weight, up_weight, gate_taps, up_taps, down_weight,
):
    edges = tree_edges()
    plan = planned(edges)
    count = len(edges)
    any_space = pl.BlockSpec(memory_space=pl.ANY)
    operands = [
        stream_in[0],
        mix_gain.reshape(1, 2048),
        lin_weight,
        branch_weight,
        lin_taps,
        rate_blocks,
        admit_blocks,
        decay_logit.reshape(1, 1024),
        mix_out_gain.reshape(1, 1024),
        out_weight.T,
        ffn_gain.reshape(1, 2048),
        gate_weight,
        up_weight,
        gate_taps,
        up_taps,
        down_weight.T,
    ]
    small = [operands[k] for k in (1, 4, 5, 6, 7, 8, 10, 13, 14)]
    dma = pltpu.SemaphoreType.DMA
    result = pl.pallas_call(
        functools.partial(kernel, edges, plan),
        out_shape=jax.ShapeDtypeStruct((LEN, 1024), BF16),
        in_specs=[any_space] * len(operands),
        out_specs=any_space,
        scratch_shapes=[
            *[pltpu.VMEM(a.shape, a.dtype) for a in small],
            pltpu.VMEM((2, 4, 4, SHARD_ROWS, 2048), BF16),
            pltpu.VMEM((2, 4, 4, SHARD_ROWS, 1024), BF16),
            pltpu.VMEM((2, 4, 4, SHARD_ROWS, 2816), BF16),
            pltpu.VMEM((2, 4, 4, SHARD_ROWS, 1408), BF16),
            pltpu.VMEM((2, LEN, 1024), BF16),
            pltpu.VMEM((2, LEN, 1024), BF16),
            pltpu.VMEM((LEN, 1024), BF16),
            pltpu.VMEM((2, 4, LEN, 256), BF16),
            pltpu.VMEM((2, 4, LEN, 256), BF16),
            pltpu.VMEM((LEN, 1408), BF16),
            pltpu.VMEM((4, LEN, 256), BF16),
            pltpu.VMEM((LEN, 1024), BF16),
            pltpu.VMEM((LEN + 8, BLOCK), F32),
            pltpu.VMEM((LEN + 8, BLOCK), F32),
            dma((count,)), dma((count,)), dma((41,)), dma((len(small),)), dma((2,)), dma((8,)), dma((8,)), dma((4,)), dma((4,)),
            dma((4,)),
        ],
        compiler_params=pltpu.CompilerParams(
            collective_id=0, has_side_effects=True, vmem_limit_bytes=63 * 1024 * 1024
        ),
    )(*operands)
    return result[None]


def solution(mesh):
    placed = (
        P(("rep", "fs"), None, "tp"), P(), P("fs", "tp"), P("fs", "tp"), P(None, "tp"), P("tp", None, None),
        P("tp", None, None), P("tp"), P("tp"), P("tp", "fs"), P(), P("fs", "tp"), P("fs", "tp"), P(None, "tp"),
        P(None, "tp"), P("tp", "fs"),
    )
    return jax.shard_map(
        local, mesh=mesh, in_specs=placed, out_specs=P(("rep", "fs"), None, "tp"), check_vma=False
    )
```

```python
import functools

import jax
import jax.numpy as jnp
from jax import lax
from jax.experimental import pallas as pl
from jax.experimental.pallas import tpu as pltpu
from jax.sharding import PartitionSpec as P

EPS = 1e-06
GATE_SCALE = 8.0
MESH = pl.DeviceIdType.MESH
F32, BF16 = jnp.float32, jnp.bfloat16

GROUPS = (
    (0, 0, (5, 5, 3, 3)),
    (1, 0, (3, 2, 1, 2)),
    (2, 0, (7, 7, 4, 4)),
    (3, 0, (3, 4, 2, 2)),
)
LINK_RATE = 48000.0
HOP_US = 3.0
EARLY_US = 100.0
GATE_UP, DOWN = (2, 2), 3
ROW_STEPS = (0, 1, -1, 2)
ROW_ORDER = tuple((half, step) for half in ("own", "other") for step in ROW_STEPS)
SHARD_ROWS = 64


def region_slots(region):
    count = 2 if region[0] == "both" else 1
    for part in region[1:]:
        if not isinstance(part, int):
            count *= part[1] - part[0]
    return count


def tree_edges():
    edges = []
    for group, (buffer, first, split) in enumerate(GROUPS):
        for tree, width in enumerate(split):
            columns = (first * 128, width * 128)
            first += width
            fast, slow = ("x", "y") if tree % 2 == 0 else ("y", "x")

            def add(name, way, region, parents):
                z, f, s = region
                placed = (z, s, f) if fast == "x" else (z, f, s)
                edges.append(
                    dict(
                        key=(group, tree, name),
                        way=way,
                        buffer=buffer,
                        region=placed,
                        columns=columns,
                        bytes=region_slots(region) * width * 128 * SHARD_ROWS * 2,
                        parents=[(group, tree, p) for p in parents],
                    )
                )

            flip = (group + tree) % 2
            one, two = ("+", "-") if flip == 0 else ("-", "+")
            if tree < 2:
                add("p+", fast + "+", ("own", 0, 0), [])
                add("p-", fast + "-", ("own", 0, 0), [])
                add("p2", fast + one, ("own", -1 if one == "+" else 1, 0), ["p" + one])
                for k, (r, par) in enumerate(((0, []), (-1, ["p+"]), (1, ["p-"]), (2, ["p2"]))):
                    add(f"q+{r}", slow + "+", ("own", r, 0), par)
                    add(f"q-{r}", slow + "-", ("own", r, 0), par)
                    a = "+" if (k + flip) % 2 else "-"
                    add(f"q2{r}", slow + a, ("own", r, -1 if a == "+" else 1), [f"q{a}{r}"])
                    za, zb = ("+", "-") if k % 2 else ("-", "+")
                    add(f"z0{r}", "z" + za, ("own", r, 0), par)
                    add(f"z1{r}", "z" + zb, ("own", r, -1), [f"q+{r}"])
                    add(f"z2{r}", "z" + za, ("own", r, 1), [f"q-{r}"])
                    add(f"z3{r}", "z" + zb, ("own", r, 2), [f"q2{r}"])
            else:
                add("z", "z" + ("+" if tree == 2 else "-"), ("own", 0, 0), [])
                for k, (z, par) in enumerate((("own", []), ("other", ["z"]))):
                    add(f"p+{z}", fast + "+", (z, 0, 0), par)
                    add(f"p-{z}", fast + "-", (z, 0, 0), par)
                    a = "+" if k else "-"
                    add(f"p2{z}", fast + a, (z, -1 if a == "+" else 1, 0), [f"p{a}{z}"])
                arrived = {
                    0: ["z"],
                    -1: ["p+own", "p+other"],
                    1: ["p-own", "p-other"],
                    2: ["p2own", "p2other"],
                }
                for k, r in enumerate((0, -1, 1, 2)):
                    add(f"q+{r}", slow + "+", ("both", r, 0), arrived[r])
                    add(f"q-{r}", slow + "-", ("both", r, 0), arrived[r])
                    a = "+" if (k + flip) % 2 else "-"
                    add(f"q2{r}", slow + a, ("both", r, -1 if a == "+" else 1), [f"q{a}{r}"])
    return edges


def landing(edge):
    z, y, x = edge["region"]
    shift = 1 if edge["way"][1] == "+" else -1
    if edge["way"][0] == "z":
        return {"own": "other", "other": "own", "both": "both"}[z], y, x
    wrap = {-2: 2, 3: -1}
    if edge["way"][0] == "y":
        return z, wrap.get(y - shift, y - shift), x
    return z, y, wrap.get(x - shift, x - shift)


def unit_of(edge):
    group, tree, name = edge["key"]
    if tree < 2 and name[0] == "z":
        return (group, tree, "z", landing(edge)[1]) if group == DOWN else (group, tree, "z")
    if tree >= 2 and name[:2] == "q2" and (group != DOWN or tree == 2):
        return (group, tree, "q2")
    return edge["key"]


def in_row(edge, row):
    z, y, _ = landing(edge)
    return z in (row[0], "both") and y == row[1]


def planned(edges):
    index = {e["key"]: k for k, e in enumerate(edges)}
    free, landed, begun = {}, {}, {}
    waiting, order = list(range(len(edges))), []
    while waiting:
        best = None
        for k in waiting:
            e = edges[k]
            if any(index[p] not in landed for p in e["parents"]):
                continue
            ready = max([landed[index[p]] for p in e["parents"]], default=0.0)
            start = max(ready, free.get(e["way"], 0.0))
            if best is None or (start, e["key"][0], ready) < best[0]:
                best = ((start, e["key"][0], ready), k, ready, start)
        _, k, ready, start = best
        free[edges[k]["way"]] = start + edges[k]["bytes"] / LINK_RATE
        landed[k] = free[edges[k]["way"]] + HOP_US
        begun[k] = (ready, start)
        waiting.remove(k)
        order.append(k)
    last, due = {}, {}
    for k in order:
        due[k] = max(begun[k][0], begun[k][1] - EARLY_US, last.get(edges[k]["way"], 0.0))
        last[edges[k]["way"]] = due[k]
    order.sort(key=lambda k: (due[k], begun[k][1]))
    return index, order, landed, due


def send_unit(edge):
    group, tree, name = edge["key"]
    return (group * 4 + tree) * 3 + "pqz".index(name[0])


class Gather:
    def __init__(self, edges, plan, buffers, send, recv):
        self.edges, self.buffers, self.send, self.recv = edges, buffers, send, recv
        self.index, self.order, self.landed, self.due = plan
        self.seen, self.queue = set(), list(self.order)
        self.unit = {}
        for e in edges:
            self.unit.setdefault(unit_of(e), len(self.unit))
        fs, rep = lax.axis_index("fs"), lax.axis_index("rep")
        x, y, half = lax.rem(fs, 4), lax.rem(lax.div(fs, 4), 4), lax.div(fs, 16)
        z = rep * 2 + half
        self.x = {r: (lax.rem(x + r + 4, 4) if r else x) for r in (-1, 0, 1, 2)}
        self.y = {r: (lax.rem(y + r + 4, 4) if r else y) for r in (-1, 0, 1, 2)}
        self.z = {"own": half, "other": 1 - half}
        self.device = {}
        for sign, d in (("+", 1), ("-", -1)):
            self.device["x" + sign] = {"fs": half * 16 + y * 4 + self.x[d]}
            self.device["y" + sign] = {"fs": half * 16 + self.y[d] * 4 + x}
            beyond = lax.rem(z + d + 4, 4)
            self.device["z" + sign] = {
                "rep": lax.div(beyond, 2),
                "fs": lax.rem(beyond, 2) * 16 + y * 4 + x,
            }

    def place(self, edge, arriving):
        z, y, x = landing(edge) if arriving else edge["region"]
        at_z = pl.ds(0, 2) if z == "both" else self.z[z]
        start, width = edge["columns"]
        return self.buffers[edge["buffer"]].at[
            at_z, self.y[y], self.x[x], :, pl.ds(start, width)
        ]

    def copy(self, k, arriving):
        edge = self.edges[k]
        ref = self.place(edge, arriving)
        return pltpu.make_async_remote_copy(
            src_ref=ref,
            dst_ref=ref,
            send_sem=self.send.at[send_unit(edge)],
            recv_sem=self.recv.at[self.unit[unit_of(edge)]],
            device_id=self.device[edge["way"]],
            device_id_type=MESH,
        )

    def whole(self, edge, at):
        start, width = edge["columns"]
        ref = self.buffers[edge["buffer"]].at[(*at, slice(None), pl.ds(start, width))]
        return pltpu.make_async_remote_copy(
            src_ref=ref,
            dst_ref=ref,
            send_sem=self.send.at[send_unit(edge)],
            recv_sem=self.recv.at[self.unit[unit_of(edge)]],
            device_id=self.device[edge["way"]],
            device_id_type=MESH,
        )

    def wait_unit(self, k):
        edge = self.edges[k]
        unit, every = unit_of(edge), pl.ds(0, 4)
        if unit == edge["key"]:
            self.copy(k, True).wait_recv()
        elif unit[2] == "z":
            self.whole(edge, (self.z["other"], self.y[unit[3]] if len(unit) > 3 else every, every)).wait_recv()
        elif unit[1] == 2:
            self.whole(edge, (pl.ds(0, 2), self.y[2], every)).wait_recv()
        else:
            self.whole(edge, (pl.ds(0, 2), every, self.x[2])).wait_recv()

    def arrivals(self, ks):
        found = []
        for k in ks:
            unit = unit_of(self.edges[k])
            if unit not in self.seen:
                self.seen.add(unit)
                found.append((True, k))
        return found

    def begin(self, k):
        return self.arrivals([self.index[p] for p in self.edges[k]["parents"]]) + [(False, k)]

    def due_by(self, until):
        steps = []
        while self.queue and self.due[self.queue[0]] <= until:
            steps += self.begin(self.queue.pop(0))
        return steps

    def members(self, group):
        return [k for k in self.order if self.edges[k]["key"][0] == group]

    def run(self, steps):
        for arriving, k in steps:
            if arriving:
                self.wait_unit(k)
            else:
                self.copy(k, False).start()

    def pump(self, until):
        self.run(self.due_by(until))

    def until_done(self, group, row=None):
        members = self.members(group)
        if row is not None:
            members = [k for k in members if in_row(self.edges[k], row)]
        steps = self.due_by(max([self.landed[k] for k in members], default=0.0) - HOP_US)
        while any(k in self.queue for k in members) or any(
            self.index[p] in self.queue for k in members for p in self.edges[k]["parents"]
        ):
            steps += self.begin(self.queue.pop(0))
        return steps + self.arrivals(members)

    def group_done(self, group):
        self.run(self.until_done(group))

    def group_time(self, group):
        return max([self.landed[k] for k in self.members(group)], default=0.0)

    def timetable(self, count, first, pace, subs=1):
        return [
            [self.due_by(first + pace * (k + j / subs)) for j in range(subs)] for k in range(count)
        ]

    def sent(self, group):
        done = set()
        for k in self.members(group):
            edge = self.edges[k]
            tree, level = edge["key"][1], edge["key"][2][0]
            if send_unit(edge) in done:
                continue
            done.add(send_unit(edge))
            half, y, x = self.z["own"], self.y[0], self.x[0]
            if tree < 2:
                at = {"p": (half, y, pl.ds(0, 3)), "q": (half, pl.ds(0, 3), pl.ds(0, 4)), "z": (half, pl.ds(0, 4), pl.ds(0, 4))}
            else:
                at = {"z": (half, y, x), "p": (pl.ds(0, 2), y, pl.ds(0, 3)), "q": (pl.ds(0, 2), pl.ds(0, 3), pl.ds(0, 4))}
            self.whole(edge, at[level]).wait_send()


def at_step(step, table, gather, sub=0):
    for k, steps in enumerate(table):
        if steps[sub]:

            @pl.when(step == k)
            def _(steps=steps[sub]):
                gather.run(steps)


def shifted_down(values, amount, fill, row):
    return jnp.where(row >= amount, pltpu.roll(values, amount, 0), fill)


def scan_rows(decay, driven, row):
    rows = decay.shape[0]
    step = 1
    while step < rows:
        before_b = shifted_down(driven, step, 0.0, row)
        before_a = shifted_down(decay, step, 1.0, row)
        driven = decay * before_b + driven
        decay = decay * before_a
        step *= 2
    return decay, driven


LEN = 768
BLOCK = 128
ROWS = 256
NORM_ROWS = 16


def kernel(edges, plan, *refs):
    (x, gain, lin, branch, taps, rate, admit, logit, mix_gain, out_w, ffn_gain, gate, up, gate_taps, up_taps, down) = refs[:16]
    result = refs[16]
    small = (gain, taps, rate, admit, logit, mix_gain, ffn_gain, gate_taps, up_taps)
    held = refs[17 : 17 + len(small)]
    (b0, b1, b2, b3, full, normed, mixed, sent, got, hidden, dgot, final, pad_a, pad_b) = refs[26:40]
    (send, recv, load, ssem, xsem, osend, orecv, dsend, drecv, fsem) = refs[40:]
    tp = lax.axis_index("tp")
    gather = Gather(edges, plan, (b0, b1, b2, b3), send, recv)
    partner = {"tp": 1 - tp}
    zl, y0, x0 = gather.z["own"], gather.y[0], gather.x[0]

    x_load = pltpu.make_async_copy(x, full.at[tp], load.at[0])
    small_loads = [pltpu.make_async_copy(a, b, ssem.at[k]) for k, (a, b) in enumerate(zip(small, held))]
    (gain, taps, rate, admit, logit, mix_gain, ffn_gain, gate_taps, up_taps) = held
    loads = []
    pieces = [(out_w, b1, 2, 0, 0, 1024), (down, b3, 4, 0, 0, 1408)]
    for k in range(8):
        pieces += [(lin, b0, 1, k * 128, k * 256, 128), (branch, b0, 1, k * 128, k * 256 + 128, 128)]
    for k in range(11):
        pieces += [(gate, b2, 3, k * 128, k * 256, 128), (up, b2, 3, k * 128, k * 256 + 128, 128)]
    for source, target, owner, at, to, width in pieces:
        loads.append(
            pltpu.make_async_copy(
                source.at[:, pl.ds(at, width)], target.at[zl, y0, x0, :, pl.ds(to, width)], load.at[owner]
            )
        )
    for one in loads:
        one.start()
    barrier = pltpu.get_barrier_semaphore()
    for device in [*gather.device.values(), partner]:
        pl.semaphore_signal(barrier, inc=1, device_id=device, device_id_type=MESH)
    pl.semaphore_wait(barrier, 7)
    x_copy = pltpu.make_async_remote_copy(
        src_ref=x, dst_ref=full.at[tp], send_sem=xsem.at[0], recv_sem=xsem.at[1], device_id=partner, device_id_type=MESH
    )
    for k, buffer in enumerate((b0, b1, b2, b3)):
        slot = buffer.at[zl, y0, x0]
        pltpu.make_async_copy(slot, slot, load.at[k + 1]).wait()
    gather.pump(0.0)
    x_copy.start()
    x_load.start()
    for one in small_loads:
        one.start()
    gather.pump(LEAD_US)
    x_load.wait()
    for one in small_loads:
        one.wait()
    x_copy.wait_send()
    pltpu.make_async_remote_copy(
        src_ref=x, dst_ref=full.at[1 - tp], send_sem=xsem.at[0], recv_sem=xsem.at[1], device_id=partner, device_id_type=MESH
    ).wait_recv()

    def norm(chunk, scales, with_sums):
        rows = pl.ds(pl.multiple_of(chunk * NORM_ROWS, NORM_ROWS), NORM_ROWS)
        halves = []
        for h in range(2):
            part = full[h, rows, :].astype(F32)
            if with_sums:
                extra = [
                    sent[h, q, rows, :].astype(F32) + got[h, q, rows, :].astype(F32) for q in range(4)
                ]
                rounded = (part + jnp.concatenate(extra, axis=1)).astype(BF16)
                full[h, rows, :] = rounded
                part = rounded.astype(F32)
            halves.append(part)
        total = sum(jnp.sum(part * part, axis=-1, keepdims=True) for part in halves)
        factor = lax.rsqrt(total * (1.0 / 2048.0) + EPS)
        for h in range(2):
            normed[h, rows, :] = (halves[h] * factor * scales[:, h * 1024 : h * 1024 + 1024]).astype(BF16)

    table = gather.timetable(LEN // NORM_ROWS // 6, *NORM_PACE)

    @pl.loop(0, LEN // NORM_ROWS // 6)
    def _(part):
        at_step(part, table, gather)

        @pl.loop(0, 6)
        def _(chunk):
            norm(part * 6 + chunk, gain, False)

    pad_a[0:8, :] = jnp.zeros((8, BLOCK), F32)
    pad_b[0:8, :] = jnp.zeros((8, BLOCK), F32)
    row = lax.broadcasted_iota(jnp.int32, (ROWS, BLOCK), 0)
    gather.group_done(0)
    start = gather.group_time(0)

    def both(buffer, step):
        columns = pl.ds(pl.multiple_of(step * 256, 256), 256)
        total = None
        for h in range(2):
            weights = buffer[h, :, :, :, columns].reshape(1024, 256)
            part = jnp.dot(normed[h], weights, preferred_element_type=F32)
            total = part if total is None else total + part
        return total.astype(BF16).astype(F32)

    table1 = gather.timetable(8, start + MIX_PACE[0], MIX_PACE[1], 4)

    @pl.loop(0, 8)
    def _(step):
        at_step(step, table1, gather, 0)
        lanes = pl.ds(pl.multiple_of(step * BLOCK, BLOCK), BLOCK)
        values = both(b0, step)
        pad_a[8 : 8 + LEN, :] = values[:, :BLOCK]
        pad_b[8 : 8 + LEN, :] = values[:, BLOCK:]
        tap = taps[:, lanes]
        base = -GATE_SCALE * jax.nn.softplus(-logit[:, lanes])
        scale = mix_gain[:, lanes]
        carry = jnp.zeros((1, BLOCK), F32)
        for c in range(LEN // ROWS):
            at_step(step, table1, gather, c + 1)
            at = c * ROWS
            filtered = sum(pad_a[5 + j + at : 5 + j + at + ROWS, :] * tap[j : j + 1, :] for j in range(4))
            rounded = filtered.astype(BF16)
            rate_gate = jax.nn.sigmoid(jnp.dot(rounded, rate[step], preferred_element_type=F32))
            admitted = jax.nn.sigmoid(jnp.dot(rounded, admit[step], preferred_element_type=F32))
            log_decay = rate_gate * base
            decay = jnp.exp(log_decay)
            rest = -jnp.tanh(log_decay) * (1.0 + decay * decay)
            driven = jnp.sqrt(rest) * admitted * filtered
            product, states = scan_rows(decay, driven, row)
            states = states + product * carry
            carry = states[ROWS - 1 : ROWS, :]
            gated = states * jax.nn.gelu(pad_b[8 + at : 8 + at + ROWS, :], approximate=True)
            mean = jnp.mean(gated * gated, axis=-1, keepdims=True)
            mixed[at : at + ROWS, lanes] = (gated * lax.rsqrt(mean + EPS) * scale).astype(BF16)

    gather.group_done(1)

    def out_copy(j):
        h, q = lax.rem(1 - tp + lax.div(j, 4), 2), lax.rem(j, 4)
        return pltpu.make_async_remote_copy(
            src_ref=sent.at[h, q], dst_ref=got.at[h, q], send_sem=osend.at[j], recv_sem=orecv.at[j],
            device_id=partner, device_id_type=MESH,
        )

    def arriving_copy(j):
        h, q = lax.rem(tp + lax.div(j, 4), 2), lax.rem(j, 4)
        return pltpu.make_async_remote_copy(
            src_ref=sent.at[h, q], dst_ref=got.at[h, q], send_sem=osend.at[j], recv_sem=orecv.at[j],
            device_id=partner, device_id_type=MESH,
        )

    table2 = gather.timetable(8, start + OUT_PACE[0], OUT_PACE[1])

    @pl.loop(0, 8)
    def _(j):
        at_step(j, table2, gather)
        h, q = lax.rem(1 - tp + lax.div(j, 4), 2), lax.rem(j, 4)
        weights = b1[h, q].reshape(256, 1024)
        part = lax.dot_general(mixed[...], weights, (((1,), (1,)), ((), ())), preferred_element_type=F32)
        sent[h, q] = part.astype(BF16)

        @pl.when(j > 0)
        def _():
            out_copy(j - 1).start()

    out_copy(7).start()
    gather.pump(start + NORM2_US)
    for j in range(8):
        arriving_copy(j).wait_recv()

    table3 = gather.timetable(LEN // NORM_ROWS // 6, start + NORM2_US, NORM_PACE[1])

    @pl.loop(0, LEN // NORM_ROWS // 6)
    def _(part):
        at_step(part, table3, gather)

        @pl.loop(0, 6)
        def _(chunk):
            norm(part * 6 + chunk, ffn_gain, True)

    for j in range(8):
        out_copy(j).wait_send()
    gather.sent(0)
    gather.group_done(GATE_UP[0])
    ready = gather.group_time(GATE_UP[0])
    table4 = gather.timetable(6, ready + FFN_PACE[0], FFN_PACE[1], 2)
    middle = gather.until_done(GATE_UP[1])
    later = max(ready + 6 * FFN_PACE[1], gather.group_time(GATE_UP[1])) + FFN_PACE[0]
    table5 = gather.timetable(5, later, FFN_PACE[1], 2)
    table4 = table4 + [[middle + table5[0][0], table5[0][1]]] + table5[1:]

    @pl.loop(0, 11)
    def _(step):
        at_step(step, table4, gather, 0)
        lanes = pl.ds(pl.multiple_of(step * BLOCK, BLOCK), BLOCK)
        values = both(b2, step)
        pad_a[8 : 8 + LEN, :] = values[:, :BLOCK]
        pad_b[8 : 8 + LEN, :] = values[:, BLOCK:]
        at_step(step, table4, gather, 1)
        tap_g, tap_u = gate_taps[:, lanes], up_taps[:, lanes]
        for c in range(LEN // ROWS):
            at = c * ROWS
            conv_g = sum(pad_a[6 + j + at : 6 + j + at + ROWS, :] * tap_g[j : j + 1, :] for j in range(3))
            conv_u = sum(pad_b[6 + j + at : 6 + j + at + ROWS, :] * tap_u[j : j + 1, :] for j in range(3))
            hidden[at : at + ROWS, lanes] = (jax.nn.silu(conv_g) * conv_u).astype(BF16)

    tables = [[gather.until_done(DOWN, row)] for row in ROW_ORDER]

    def row_of(j):
        k = lax.rem(j, 4)
        step = jnp.where(k == 2, 3, jnp.where(k == 3, 2, k))
        return lax.rem(zl + lax.div(j, 4), 2), lax.rem(y0 + step, 4)

    def down_copy(q):
        return pltpu.make_async_remote_copy(
            src_ref=sent.at[0, q], dst_ref=dgot.at[q], send_sem=dsend.at[q], recv_sem=drecv.at[q],
            device_id=partner, device_id_type=MESH,
        )

    def final_copy(q):
        lanes = pl.ds(pl.multiple_of(q * 256, 256), 256)
        return pltpu.make_async_copy(final.at[:, lanes], result.at[:, lanes], fsem.at[q])

    def complete(j):
        _, q = row_of(j)
        down_copy(q).wait_recv()
        lanes = pl.ds(pl.multiple_of(q * 256, 256), 256)
        total = sent[1, q].astype(F32) + dgot[q].astype(F32)
        final[:, lanes] = (full[tp, :, lanes].astype(F32) + total).astype(BF16)
        final_copy(q).start()

    def pass_on(j):
        h, q = row_of(j)

        @pl.when(h != tp)
        def _():
            down_copy(q).start()

    @pl.loop(0, 8)
    def _(j):
        at_step(j, tables, gather)
        h, q = row_of(j)
        weights = b3[h, q].reshape(256, 1408)
        part = lax.dot_general(hidden[...], weights, (((1,), (1,)), ((), ())), preferred_element_type=F32)
        sent[jnp.where(h == tp, 1, 0), q] = part.astype(BF16)

        @pl.when(j > 0)
        def _():
            pass_on(j - 1)

        @pl.when(j >= 6)
        def _():
            complete(j - 6)

    pass_on(7)
    gather.pump(1e9)
    for group in range(1, DOWN):
        gather.sent(group)
    complete(2)
    complete(3)
    gather.sent(DOWN)
    for q in range(4):
        down_copy(q).wait_send()
        final_copy(q).wait()


LEAD_US = 3.0
NORM_PACE = (3.0, 0.9)
MIX_PACE = (4.0, 3.0)
OUT_PACE = (28.0, 0.8)
NORM2_US = 37.0
FFN_PACE = (4.0, 1.6)


def local(
    stream_in, mix_gain, lin_weight, branch_weight, lin_taps, rate_blocks, admit_blocks, decay_logit, mix_out_gain,
    out_weight, ffn_gain, gate_weight, up_weight, gate_taps, up_taps, down_weight,
):
    edges = tree_edges()
    plan = planned(edges)
    count, sends = len({unit_of(e) for e in edges}), 12 * len(GROUPS)
    any_space = pl.BlockSpec(memory_space=pl.ANY)
    operands = [
        stream_in[0],
        mix_gain.reshape(1, 2048),
        lin_weight,
        branch_weight,
        lin_taps,
        rate_blocks,
        admit_blocks,
        decay_logit.reshape(1, 1024),
        mix_out_gain.reshape(1, 1024),
        out_weight.T,
        ffn_gain.reshape(1, 2048),
        gate_weight,
        up_weight,
        gate_taps,
        up_taps,
        down_weight.T,
    ]
    small = [operands[k] for k in (1, 4, 5, 6, 7, 8, 10, 13, 14)]
    dma = pltpu.SemaphoreType.DMA
    result = pl.pallas_call(
        functools.partial(kernel, edges, plan),
        out_shape=jax.ShapeDtypeStruct((LEN, 1024), BF16),
        in_specs=[any_space] * len(operands),
        out_specs=any_space,
        scratch_shapes=[
            *[pltpu.VMEM(a.shape, a.dtype) for a in small],
            pltpu.VMEM((2, 4, 4, SHARD_ROWS, 2048), BF16),
            pltpu.VMEM((2, 4, 4, SHARD_ROWS, 1024), BF16),
            pltpu.VMEM((2, 4, 4, SHARD_ROWS, 2816), BF16),
            pltpu.VMEM((2, 4, 4, SHARD_ROWS, 1408), BF16),
            pltpu.VMEM((2, LEN, 1024), BF16),
            pltpu.VMEM((2, LEN, 1024), BF16),
            pltpu.VMEM((LEN, 1024), BF16),
            pltpu.VMEM((2, 4, LEN, 256), BF16),
            pltpu.VMEM((2, 4, LEN, 256), BF16),
            pltpu.VMEM((LEN, 1408), BF16),
            pltpu.VMEM((4, LEN, 256), BF16),
            pltpu.VMEM((LEN, 1024), BF16),
            pltpu.VMEM((LEN + 8, BLOCK), F32),
            pltpu.VMEM((LEN + 8, BLOCK), F32),
            dma((sends,)), dma((count,)), dma((5,)), dma((len(small),)), dma((2,)), dma((8,)), dma((8,)), dma((4,)), dma((4,)),
            dma((4,)),
        ],
        compiler_params=pltpu.CompilerParams(
            collective_id=0, has_side_effects=True, vmem_limit_bytes=63 * 1024 * 1024
        ),
    )(*operands)
    return result[None]


def solution(mesh):
    placed = (
        P(("rep", "fs"), None, "tp"), P(), P("fs", "tp"), P("fs", "tp"), P(None, "tp"), P("tp", None, None),
        P("tp", None, None), P("tp"), P("tp"), P("tp", "fs"), P(), P("fs", "tp"), P("fs", "tp"), P(None, "tp"),
        P(None, "tp"), P("tp", "fs"),
    )
    return jax.shard_map(
        local, mesh=mesh, in_specs=placed, out_specs=P(("rep", "fs"), None, "tp"), check_vma=False
    )
```

```python
import functools

import jax
import jax.numpy as jnp
from jax import lax
from jax.experimental import pallas as pl
from jax.experimental.pallas import tpu as pltpu
from jax.sharding import PartitionSpec as P

EPS = 1e-06
GATE_SCALE = 8.0
MESH = pl.DeviceIdType.MESH
F32, BF16 = jnp.float32, jnp.bfloat16

GROUPS = (
    (0, 0, (5, 5, 3, 3)),
    (1, 0, (3, 2, 1, 2)),
    (2, 0, (7, 7, 4, 4)),
    (3, 0, (3, 4, 2, 2)),
)
LINK_RATE = 48000.0
HOP_US = 3.0
EARLY_US = 100.0
GATE_UP, DOWN = (2, 2), 3
ROW_STEPS = (0, 1, -1, 2)
ROW_ORDER = tuple((half, step) for half in ("own", "other") for step in ROW_STEPS)
SHARD_ROWS = 64


def region_slots(region):
    count = 2 if region[0] == "both" else 1
    for part in region[1:]:
        if not isinstance(part, int):
            count *= part[1] - part[0]
    return count


def tree_edges():
    edges = []
    for group, (buffer, first, split) in enumerate(GROUPS):
        for tree, width in enumerate(split):
            columns = (first * 128, width * 128)
            first += width
            fast, slow = ("x", "y") if tree % 2 == 0 else ("y", "x")

            def add(name, way, region, parents):
                z, f, s = region
                placed = (z, s, f) if fast == "x" else (z, f, s)
                edges.append(
                    dict(
                        key=(group, tree, name),
                        way=way,
                        buffer=buffer,
                        region=placed,
                        columns=columns,
                        bytes=region_slots(region) * width * 128 * SHARD_ROWS * 2,
                        parents=[(group, tree, p) for p in parents],
                    )
                )

            flip = (group + tree) % 2
            one, two = ("+", "-") if flip == 0 else ("-", "+")
            if tree < 2:
                add("p+", fast + "+", ("own", 0, 0), [])
                add("p-", fast + "-", ("own", 0, 0), [])
                add("p2", fast + one, ("own", -1 if one == "+" else 1, 0), ["p" + one])
                for k, (r, par) in enumerate(((0, []), (-1, ["p+"]), (1, ["p-"]), (2, ["p2"]))):
                    add(f"q+{r}", slow + "+", ("own", r, 0), par)
                    add(f"q-{r}", slow + "-", ("own", r, 0), par)
                    a = "+" if (k + flip) % 2 else "-"
                    add(f"q2{r}", slow + a, ("own", r, -1 if a == "+" else 1), [f"q{a}{r}"])
                    za, zb = ("+", "-") if k % 2 else ("-", "+")
                    add(f"z0{r}", "z" + za, ("own", r, 0), par)
                    add(f"z1{r}", "z" + zb, ("own", r, -1), [f"q+{r}"])
                    add(f"z2{r}", "z" + za, ("own", r, 1), [f"q-{r}"])
                    add(f"z3{r}", "z" + zb, ("own", r, 2), [f"q2{r}"])
            else:
                add("z", "z" + ("+" if tree == 2 else "-"), ("own", 0, 0), [])
                for k, (z, par) in enumerate((("own", []), ("other", ["z"]))):
                    add(f"p+{z}", fast + "+", (z, 0, 0), par)
                    add(f"p-{z}", fast + "-", (z, 0, 0), par)
                    a = "+" if k else "-"
                    add(f"p2{z}", fast + a, (z, -1 if a == "+" else 1, 0), [f"p{a}{z}"])
                arrived = {
                    0: ["z"],
                    -1: ["p+own", "p+other"],
                    1: ["p-own", "p-other"],
                    2: ["p2own", "p2other"],
                }
                for k, r in enumerate((0, -1, 1, 2)):
                    add(f"q+{r}", slow + "+", ("both", r, 0), arrived[r])
                    add(f"q-{r}", slow + "-", ("both", r, 0), arrived[r])
                    a = "+" if (k + flip) % 2 else "-"
                    add(f"q2{r}", slow + a, ("both", r, -1 if a == "+" else 1), [f"q{a}{r}"])
    return edges


def landing(edge):
    z, y, x = edge["region"]
    shift = 1 if edge["way"][1] == "+" else -1
    if edge["way"][0] == "z":
        return {"own": "other", "other": "own", "both": "both"}[z], y, x
    wrap = {-2: 2, 3: -1}
    if edge["way"][0] == "y":
        return z, wrap.get(y - shift, y - shift), x
    return z, y, wrap.get(x - shift, x - shift)


def unit_of(edge):
    group, tree, name = edge["key"]
    if tree < 2 and name[0] == "z":
        return (group, tree, "z", landing(edge)[1]) if group == DOWN else (group, tree, "z")
    if tree >= 2 and name[:2] == "q2" and (group != DOWN or tree == 2):
        return (group, tree, "q2")
    return edge["key"]


def in_row(edge, row):
    z, y, _ = landing(edge)
    return z in (row[0], "both") and y == row[1]


def planned(edges):
    index = {e["key"]: k for k, e in enumerate(edges)}
    free, landed, begun = {}, {}, {}
    waiting, order = list(range(len(edges))), []
    while waiting:
        best = None
        for k in waiting:
            e = edges[k]
            if any(index[p] not in landed for p in e["parents"]):
                continue
            ready = max([landed[index[p]] for p in e["parents"]], default=0.0)
            start = max(ready, free.get(e["way"], 0.0))
            if best is None or (start, e["key"][0], ready) < best[0]:
                best = ((start, e["key"][0], ready), k, ready, start)
        _, k, ready, start = best
        free[edges[k]["way"]] = start + edges[k]["bytes"] / LINK_RATE
        landed[k] = free[edges[k]["way"]] + HOP_US
        begun[k] = (ready, start)
        waiting.remove(k)
        order.append(k)
    last, due = {}, {}
    for k in order:
        due[k] = max(begun[k][0], begun[k][1] - EARLY_US, last.get(edges[k]["way"], 0.0))
        last[edges[k]["way"]] = due[k]
    order.sort(key=lambda k: (due[k], begun[k][1]))
    return index, order, landed, due


def send_unit(edge):
    group, tree, name = edge["key"]
    return (group * 4 + tree) * 3 + "pqz".index(name[0])


class Gather:
    def __init__(self, edges, plan, buffers, send, recv):
        self.edges, self.buffers, self.send, self.recv = edges, buffers, send, recv
        self.index, self.order, self.landed, self.due = plan
        self.seen, self.queue = set(), list(self.order)
        self.unit = {}
        for e in edges:
            self.unit.setdefault(unit_of(e), len(self.unit))
        fs, rep = lax.axis_index("fs"), lax.axis_index("rep")
        x, y, half = lax.rem(fs, 4), lax.rem(lax.div(fs, 4), 4), lax.div(fs, 16)
        z = rep * 2 + half
        self.x = {r: (lax.rem(x + r + 4, 4) if r else x) for r in (-1, 0, 1, 2)}
        self.y = {r: (lax.rem(y + r + 4, 4) if r else y) for r in (-1, 0, 1, 2)}
        self.z = {"own": half, "other": 1 - half}
        self.device = {}
        for sign, d in (("+", 1), ("-", -1)):
            self.device["x" + sign] = {"fs": half * 16 + y * 4 + self.x[d]}
            self.device["y" + sign] = {"fs": half * 16 + self.y[d] * 4 + x}
            beyond = lax.rem(z + d + 4, 4)
            self.device["z" + sign] = {
                "rep": lax.div(beyond, 2),
                "fs": lax.rem(beyond, 2) * 16 + y * 4 + x,
            }

    def place(self, edge, arriving):
        z, y, x = landing(edge) if arriving else edge["region"]
        at_z = pl.ds(0, 2) if z == "both" else self.z[z]
        start, width = edge["columns"]
        return self.buffers[edge["buffer"]].at[
            at_z, self.y[y], self.x[x], :, pl.ds(start, width)
        ]

    def copy(self, k, arriving):
        edge = self.edges[k]
        ref = self.place(edge, arriving)
        return pltpu.make_async_remote_copy(
            src_ref=ref,
            dst_ref=ref,
            send_sem=self.send.at[send_unit(edge)],
            recv_sem=self.recv.at[self.unit[unit_of(edge)]],
            device_id=self.device[edge["way"]],
            device_id_type=MESH,
        )

    def whole(self, edge, at):
        start, width = edge["columns"]
        ref = self.buffers[edge["buffer"]].at[(*at, slice(None), pl.ds(start, width))]
        return pltpu.make_async_remote_copy(
            src_ref=ref,
            dst_ref=ref,
            send_sem=self.send.at[send_unit(edge)],
            recv_sem=self.recv.at[self.unit[unit_of(edge)]],
            device_id=self.device[edge["way"]],
            device_id_type=MESH,
        )

    def wait_unit(self, k):
        edge = self.edges[k]
        unit, every = unit_of(edge), pl.ds(0, 4)
        if unit == edge["key"]:
            self.copy(k, True).wait_recv()
        elif unit[2] == "z":
            self.whole(edge, (self.z["other"], self.y[unit[3]] if len(unit) > 3 else every, every)).wait_recv()
        elif unit[1] == 2:
            self.whole(edge, (pl.ds(0, 2), self.y[2], every)).wait_recv()
        else:
            self.whole(edge, (pl.ds(0, 2), every, self.x[2])).wait_recv()

    def arrivals(self, ks):
        found = []
        for k in ks:
            unit = unit_of(self.edges[k])
            if unit not in self.seen:
                self.seen.add(unit)
                found.append((True, k))
        return found

    def begin(self, k):
        return self.arrivals([self.index[p] for p in self.edges[k]["parents"]]) + [(False, k)]

    def due_by(self, until):
        steps = []
        while self.queue and self.due[self.queue[0]] <= until:
            steps += self.begin(self.queue.pop(0))
        return steps

    def members(self, group):
        return [k for k in self.order if self.edges[k]["key"][0] == group]

    def run(self, steps):
        for arriving, k in steps:
            if arriving:
                self.wait_unit(k)
            else:
                self.copy(k, False).start()

    def pump(self, until):
        self.run(self.due_by(until))

    def until_done(self, group, row=None):
        members = self.members(group)
        if row is not None:
            members = [k for k in members if in_row(self.edges[k], row)]
        steps = self.due_by(max([self.landed[k] for k in members], default=0.0) - HOP_US)
        while any(k in self.queue for k in members) or any(
            self.index[p] in self.queue for k in members for p in self.edges[k]["parents"]
        ):
            steps += self.begin(self.queue.pop(0))
        return steps + self.arrivals(members)

    def group_done(self, group):
        self.run(self.until_done(group))

    def group_time(self, group):
        return max([self.landed[k] for k in self.members(group)], default=0.0)

    def timetable(self, count, first, pace, subs=1):
        return [
            [self.due_by(first + pace * (k + j / subs)) for j in range(subs)] for k in range(count)
        ]

    def sent(self, group):
        done = set()
        for k in self.members(group):
            edge = self.edges[k]
            tree, level = edge["key"][1], edge["key"][2][0]
            if send_unit(edge) in done:
                continue
            done.add(send_unit(edge))
            half, y, x = self.z["own"], self.y[0], self.x[0]
            if tree < 2:
                at = {"p": (half, y, pl.ds(0, 3)), "q": (half, pl.ds(0, 3), pl.ds(0, 4)), "z": (half, pl.ds(0, 4), pl.ds(0, 4))}
            else:
                at = {"z": (half, y, x), "p": (pl.ds(0, 2), y, pl.ds(0, 3)), "q": (pl.ds(0, 2), pl.ds(0, 3), pl.ds(0, 4))}
            self.whole(edge, at[level]).wait_send()


def at_step(step, table, gather, sub=0):
    for k, steps in enumerate(table):
        if steps[sub]:

            @pl.when(step == k)
            def _(steps=steps[sub]):
                gather.run(steps)


def shifted_down(values, amount, fill, row):
    return jnp.where(row >= amount, pltpu.roll(values, amount, 0), fill)


def scan_rows(decay, driven, row):
    rows = decay.shape[0]
    step = 1
    while step < rows:
        before_b = shifted_down(driven, step, 0.0, row)
        before_a = shifted_down(decay, step, 1.0, row)
        driven = decay * before_b + driven
        decay = decay * before_a
        step *= 2
    return decay, driven


LEN = 768
BLOCK = 128
ROWS = 256
NORM_ROWS = 16


def kernel(edges, plan, *refs):
    (x, gain, lin, branch, taps, rate, admit, logit, mix_gain, out_w, ffn_gain, gate, up, gate_taps, up_taps, down) = refs[:16]
    result = refs[16]
    small = (gain, taps, rate, admit, logit, mix_gain, ffn_gain, gate_taps, up_taps)
    held = refs[17 : 17 + len(small)]
    (b0, b1, b2, b3, full, normed, mixed, sent, got, hidden, dgot, final, pad_a, pad_b) = refs[26:40]
    (send, recv, load, ssem, xsem, osend, orecv, dsend, drecv, fsem) = refs[40:]
    tp = lax.axis_index("tp")
    gather = Gather(edges, plan, (b0, b1, b2, b3), send, recv)
    partner = {"tp": 1 - tp}
    zl, y0, x0 = gather.z["own"], gather.y[0], gather.x[0]

    x_load = pltpu.make_async_copy(x, full.at[tp], load.at[0])
    small_loads = [pltpu.make_async_copy(a, b, ssem.at[k]) for k, (a, b) in enumerate(zip(small, held))]
    (gain, taps, rate, admit, logit, mix_gain, ffn_gain, gate_taps, up_taps) = held
    loads = []
    pieces = [(out_w, b1, 2, 0, 0, 1024), (down, b3, 4, 0, 0, 1408)]
    for k in range(8):
        pieces += [(lin, b0, 1, k * 128, k * 256, 128), (branch, b0, 1, k * 128, k * 256 + 128, 128)]
    for k in range(11):
        pieces += [(gate, b2, 3, k * 128, k * 256, 128), (up, b2, 3, k * 128, k * 256 + 128, 128)]
    for source, target, owner, at, to, width in pieces:
        loads.append(
            pltpu.make_async_copy(
                source.at[:, pl.ds(at, width)], target.at[zl, y0, x0, :, pl.ds(to, width)], load.at[owner]
            )
        )
    for one in loads:
        one.start()
    barrier = pltpu.get_barrier_semaphore()
    for device in [*gather.device.values(), partner]:
        pl.semaphore_signal(barrier, inc=1, device_id=device, device_id_type=MESH)
    pl.semaphore_wait(barrier, 7)
    x_copy = pltpu.make_async_remote_copy(
        src_ref=x, dst_ref=full.at[tp], send_sem=xsem.at[0], recv_sem=xsem.at[1], device_id=partner, device_id_type=MESH
    )
    for k, buffer in enumerate((b0, b1, b2, b3)):
        slot = buffer.at[zl, y0, x0]
        pltpu.make_async_copy(slot, slot, load.at[k + 1]).wait()
    gather.pump(0.0)
    x_copy.start()
    x_load.start()
    for one in small_loads:
        one.start()
    gather.pump(LEAD_US)
    x_load.wait()
    for one in small_loads:
        one.wait()
    x_copy.wait_send()
    pltpu.make_async_remote_copy(
        src_ref=x, dst_ref=full.at[1 - tp], send_sem=xsem.at[0], recv_sem=xsem.at[1], device_id=partner, device_id_type=MESH
    ).wait_recv()

    def norm(chunk, scales, with_sums):
        rows = pl.ds(pl.multiple_of(chunk * NORM_ROWS, NORM_ROWS), NORM_ROWS)
        halves = []
        for h in range(2):
            part = full[h, rows, :].astype(F32)
            if with_sums:
                extra = [
                    sent[h, q, rows, :].astype(F32) + got[h, q, rows, :].astype(F32) for q in range(4)
                ]
                rounded = (part + jnp.concatenate(extra, axis=1)).astype(BF16)
                full[h, rows, :] = rounded
                part = rounded.astype(F32)
            halves.append(part)
        total = sum(jnp.sum(part * part, axis=-1, keepdims=True) for part in halves)
        factor = lax.rsqrt(total * (1.0 / 2048.0) + EPS)
        for h in range(2):
            normed[rows, h * 1024 : h * 1024 + 1024] = (halves[h] * factor * scales[:, h * 1024 : h * 1024 + 1024]).astype(BF16)

    table = gather.timetable(LEN // NORM_ROWS // 6, *NORM_PACE)

    @pl.loop(0, LEN // NORM_ROWS // 6)
    def _(part):
        at_step(part, table, gather)

        @pl.loop(0, 6)
        def _(chunk):
            norm(part * 6 + chunk, gain, False)

    pad_a[0:8, :] = jnp.zeros((8, BLOCK), F32)
    pad_b[0:8, :] = jnp.zeros((8, BLOCK), F32)
    row = lax.broadcasted_iota(jnp.int32, (ROWS, BLOCK), 0)
    gather.group_done(0)
    start = gather.group_time(0)

    def both(buffer, step):
        columns = pl.ds(pl.multiple_of(step * 256, 256), 256)
        weights = buffer[:, :, :, :, columns].reshape(2048, 256)
        total = jnp.dot(normed[...], weights, preferred_element_type=F32)
        return total.astype(BF16).astype(F32)

    table1 = gather.timetable(8, start + MIX_PACE[0], MIX_PACE[1], 4)

    @pl.loop(0, 8)
    def _(step):
        at_step(step, table1, gather, 0)
        lanes = pl.ds(pl.multiple_of(step * BLOCK, BLOCK), BLOCK)
        values = both(b0, step)
        pad_a[8 : 8 + LEN, :] = values[:, :BLOCK]
        pad_b[8 : 8 + LEN, :] = values[:, BLOCK:]
        tap = taps[:, lanes]
        base = -GATE_SCALE * jax.nn.softplus(-logit[:, lanes])
        scale = mix_gain[:, lanes]
        carry = jnp.zeros((1, BLOCK), F32)
        for c in range(LEN // ROWS):
            at_step(step, table1, gather, c + 1)
            at = c * ROWS
            filtered = sum(pad_a[5 + j + at : 5 + j + at + ROWS, :] * tap[j : j + 1, :] for j in range(4))
            rounded = filtered.astype(BF16)
            rate_gate = jax.nn.sigmoid(jnp.dot(rounded, rate[step], preferred_element_type=F32))
            admitted = jax.nn.sigmoid(jnp.dot(rounded, admit[step], preferred_element_type=F32))
            log_decay = rate_gate * base
            decay = jnp.exp(log_decay)
            rest = -jnp.tanh(log_decay) * (1.0 + decay * decay)
            driven = jnp.sqrt(rest) * admitted * filtered
            product, states = scan_rows(decay, driven, row)
            states = states + product * carry
            carry = states[ROWS - 1 : ROWS, :]
            gated = states * jax.nn.gelu(pad_b[8 + at : 8 + at + ROWS, :], approximate=True)
            mean = jnp.mean(gated * gated, axis=-1, keepdims=True)
            mixed[at : at + ROWS, lanes] = (gated * lax.rsqrt(mean + EPS) * scale).astype(BF16)

    gather.group_done(1)

    def out_copy(j):
        h, q = lax.rem(1 - tp + lax.div(j, 4), 2), lax.rem(j, 4)
        return pltpu.make_async_remote_copy(
            src_ref=sent.at[h, q], dst_ref=got.at[h, q], send_sem=osend.at[j], recv_sem=orecv.at[j],
            device_id=partner, device_id_type=MESH,
        )

    def arriving_copy(j):
        h, q = lax.rem(tp + lax.div(j, 4), 2), lax.rem(j, 4)
        return pltpu.make_async_remote_copy(
            src_ref=sent.at[h, q], dst_ref=got.at[h, q], send_sem=osend.at[j], recv_sem=orecv.at[j],
            device_id=partner, device_id_type=MESH,
        )

    table2 = gather.timetable(8, start + OUT_PACE[0], OUT_PACE[1])

    @pl.loop(0, 8)
    def _(j):
        at_step(j, table2, gather)
        h, q = lax.rem(1 - tp + lax.div(j, 4), 2), lax.rem(j, 4)
        weights = b1[h, q].reshape(256, 1024)
        part = lax.dot_general(mixed[...], weights, (((1,), (1,)), ((), ())), preferred_element_type=F32)
        sent[h, q] = part.astype(BF16)

        @pl.when(j > 0)
        def _():
            out_copy(j - 1).start()

    out_copy(7).start()
    gather.pump(start + NORM2_US)
    for j in range(8):
        arriving_copy(j).wait_recv()

    table3 = gather.timetable(LEN // NORM_ROWS // 6, start + NORM2_US, NORM_PACE[1])

    @pl.loop(0, LEN // NORM_ROWS // 6)
    def _(part):
        at_step(part, table3, gather)

        @pl.loop(0, 6)
        def _(chunk):
            norm(part * 6 + chunk, ffn_gain, True)

    for j in range(8):
        out_copy(j).wait_send()
    gather.sent(0)
    gather.group_done(GATE_UP[0])
    ready = gather.group_time(GATE_UP[0])
    table4 = gather.timetable(6, ready + FFN_PACE[0], FFN_PACE[1], 2)
    middle = gather.until_done(GATE_UP[1])
    later = max(ready + 6 * FFN_PACE[1], gather.group_time(GATE_UP[1])) + FFN_PACE[0]
    table5 = gather.timetable(5, later, FFN_PACE[1], 2)
    table4 = table4 + [[middle + table5[0][0], table5[0][1]]] + table5[1:]

    @pl.loop(0, 11)
    def _(step):
        at_step(step, table4, gather, 0)
        lanes = pl.ds(pl.multiple_of(step * BLOCK, BLOCK), BLOCK)
        values = both(b2, step)
        pad_a[8 : 8 + LEN, :] = values[:, :BLOCK]
        pad_b[8 : 8 + LEN, :] = values[:, BLOCK:]
        at_step(step, table4, gather, 1)
        tap_g, tap_u = gate_taps[:, lanes], up_taps[:, lanes]
        for c in range(LEN // ROWS):
            at = c * ROWS
            conv_g = sum(pad_a[6 + j + at : 6 + j + at + ROWS, :] * tap_g[j : j + 1, :] for j in range(3))
            conv_u = sum(pad_b[6 + j + at : 6 + j + at + ROWS, :] * tap_u[j : j + 1, :] for j in range(3))
            hidden[at : at + ROWS, lanes] = (jax.nn.silu(conv_g) * conv_u).astype(BF16)

    tables = [[gather.until_done(DOWN, row)] for row in ROW_ORDER]

    def row_of(j):
        k = lax.rem(j, 4)
        step = jnp.where(k == 2, 3, jnp.where(k == 3, 2, k))
        return lax.rem(zl + lax.div(j, 4), 2), lax.rem(y0 + step, 4)

    def down_copy(q):
        return pltpu.make_async_remote_copy(
            src_ref=sent.at[0, q], dst_ref=dgot.at[q], send_sem=dsend.at[q], recv_sem=drecv.at[q],
            device_id=partner, device_id_type=MESH,
        )

    def final_copy(q):
        lanes = pl.ds(pl.multiple_of(q * 256, 256), 256)
        return pltpu.make_async_copy(final.at[:, lanes], result.at[:, lanes], fsem.at[q])

    def complete(j):
        _, q = row_of(j)
        down_copy(q).wait_recv()
        lanes = pl.ds(pl.multiple_of(q * 256, 256), 256)
        total = sent[1, q].astype(F32) + dgot[q].astype(F32)
        final[:, lanes] = (full[tp, :, lanes].astype(F32) + total).astype(BF16)
        final_copy(q).start()

    def pass_on(j):
        h, q = row_of(j)

        @pl.when(h != tp)
        def _():
            down_copy(q).start()

    @pl.loop(0, 8)
    def _(j):
        at_step(j, tables, gather)
        h, q = row_of(j)
        weights = b3[h, q].reshape(256, 1408)
        part = lax.dot_general(hidden[...], weights, (((1,), (1,)), ((), ())), preferred_element_type=F32)
        sent[jnp.where(h == tp, 1, 0), q] = part.astype(BF16)

        @pl.when(j > 0)
        def _():
            pass_on(j - 1)

        @pl.when(j >= 6)
        def _():
            complete(j - 6)

    pass_on(7)
    gather.pump(1e9)
    for group in range(1, DOWN):
        gather.sent(group)
    complete(2)
    complete(3)
    gather.sent(DOWN)
    for q in range(4):
        down_copy(q).wait_send()
        final_copy(q).wait()


LEAD_US = 3.0
NORM_PACE = (3.0, 0.9)
MIX_PACE = (4.0, 3.0)
OUT_PACE = (28.0, 0.8)
NORM2_US = 37.0
FFN_PACE = (3.0, 1.4)


def local(
    stream_in, mix_gain, lin_weight, branch_weight, lin_taps, rate_blocks, admit_blocks, decay_logit, mix_out_gain,
    out_weight, ffn_gain, gate_weight, up_weight, gate_taps, up_taps, down_weight,
):
    edges = tree_edges()
    plan = planned(edges)
    count, sends = len({unit_of(e) for e in edges}), 12 * len(GROUPS)
    any_space = pl.BlockSpec(memory_space=pl.ANY)
    operands = [
        stream_in[0],
        mix_gain.reshape(1, 2048),
        lin_weight,
        branch_weight,
        lin_taps,
        rate_blocks,
        admit_blocks,
        decay_logit.reshape(1, 1024),
        mix_out_gain.reshape(1, 1024),
        out_weight.T,
        ffn_gain.reshape(1, 2048),
        gate_weight,
        up_weight,
        gate_taps,
        up_taps,
        down_weight.T,
    ]
    small = [operands[k] for k in (1, 4, 5, 6, 7, 8, 10, 13, 14)]
    dma = pltpu.SemaphoreType.DMA
    result = pl.pallas_call(
        functools.partial(kernel, edges, plan),
        out_shape=jax.ShapeDtypeStruct((LEN, 1024), BF16),
        in_specs=[any_space] * len(operands),
        out_specs=any_space,
        scratch_shapes=[
            *[pltpu.VMEM(a.shape, a.dtype) for a in small],
            pltpu.VMEM((2, 4, 4, SHARD_ROWS, 2048), BF16),
            pltpu.VMEM((2, 4, 4, SHARD_ROWS, 1024), BF16),
            pltpu.VMEM((2, 4, 4, SHARD_ROWS, 2816), BF16),
            pltpu.VMEM((2, 4, 4, SHARD_ROWS, 1408), BF16),
            pltpu.VMEM((2, LEN, 1024), BF16),
            pltpu.VMEM((LEN, 2048), BF16),
            pltpu.VMEM((LEN, 1024), BF16),
            pltpu.VMEM((2, 4, LEN, 256), BF16),
            pltpu.VMEM((2, 4, LEN, 256), BF16),
            pltpu.VMEM((LEN, 1408), BF16),
            pltpu.VMEM((4, LEN, 256), BF16),
            pltpu.VMEM((LEN, 1024), BF16),
            pltpu.VMEM((LEN + 8, BLOCK), F32),
            pltpu.VMEM((LEN + 8, BLOCK), F32),
            dma((sends,)), dma((count,)), dma((5,)), dma((len(small),)), dma((2,)), dma((8,)), dma((8,)), dma((4,)), dma((4,)),
            dma((4,)),
        ],
        compiler_params=pltpu.CompilerParams(
            collective_id=0, has_side_effects=True, vmem_limit_bytes=63 * 1024 * 1024
        ),
    )(*operands)
    return result[None]


def solution(mesh):
    placed = (
        P(("rep", "fs"), None, "tp"), P(), P("fs", "tp"), P("fs", "tp"), P(None, "tp"), P("tp", None, None),
        P("tp", None, None), P("tp"), P("tp"), P("tp", "fs"), P(), P("fs", "tp"), P("fs", "tp"), P(None, "tp"),
        P(None, "tp"), P("tp", "fs"),
    )
    return jax.shard_map(
        local, mesh=mesh, in_specs=placed, out_specs=P(("rep", "fs"), None, "tp"), check_vma=False
    )
```

```python
import functools

import jax
import jax.numpy as jnp
from jax import lax
from jax.experimental import pallas as pl
from jax.experimental.pallas import tpu as pltpu
from jax.sharding import PartitionSpec as P

EPS = 1e-06
GATE_SCALE = 8.0
MESH = pl.DeviceIdType.MESH
F32, BF16 = jnp.float32, jnp.bfloat16

GROUPS = (
    (0, 0, (5, 5, 3, 3)),
    (1, 0, (3, 2, 1, 2)),
    (2, 0, (7, 7, 4, 4)),
    (3, 0, (3, 4, 2, 2)),
)
LINK_RATE = 48000.0
HOP_US = 3.0
EARLY_US = 100.0
GATE_UP, DOWN = (2, 2), 3
ROW_STEPS = (0, 1, -1, 2)
ROW_ORDER = tuple((half, step) for half in ("own", "other") for step in ROW_STEPS)
SHARD_ROWS = 64


def region_slots(region):
    count = 2 if region[0] == "both" else 1
    for part in region[1:]:
        if not isinstance(part, int):
            count *= part[1] - part[0]
    return count


def tree_edges():
    edges = []
    for group, (buffer, first, split) in enumerate(GROUPS):
        for tree, width in enumerate(split):
            columns = (first * 128, width * 128)
            first += width
            fast, slow = ("x", "y") if tree % 2 == 0 else ("y", "x")

            def add(name, way, region, parents):
                z, f, s = region
                placed = (z, s, f) if fast == "x" else (z, f, s)
                edges.append(
                    dict(
                        key=(group, tree, name),
                        way=way,
                        buffer=buffer,
                        region=placed,
                        columns=columns,
                        bytes=region_slots(region) * width * 128 * SHARD_ROWS * 2,
                        parents=[(group, tree, p) for p in parents],
                    )
                )

            flip = (group + tree) % 2
            one, two = ("+", "-") if flip == 0 else ("-", "+")
            if tree < 2:
                add("p+", fast + "+", ("own", 0, 0), [])
                add("p-", fast + "-", ("own", 0, 0), [])
                add("p2", fast + one, ("own", -1 if one == "+" else 1, 0), ["p" + one])
                for k, (r, par) in enumerate(((0, []), (-1, ["p+"]), (1, ["p-"]), (2, ["p2"]))):
                    add(f"q+{r}", slow + "+", ("own", r, 0), par)
                    add(f"q-{r}", slow + "-", ("own", r, 0), par)
                    a = "+" if (k + flip) % 2 else "-"
                    add(f"q2{r}", slow + a, ("own", r, -1 if a == "+" else 1), [f"q{a}{r}"])
                    za, zb = ("+", "-") if k % 2 else ("-", "+")
                    add(f"z0{r}", "z" + za, ("own", r, 0), par)
                    add(f"z1{r}", "z" + zb, ("own", r, -1), [f"q+{r}"])
                    add(f"z2{r}", "z" + za, ("own", r, 1), [f"q-{r}"])
                    add(f"z3{r}", "z" + zb, ("own", r, 2), [f"q2{r}"])
            else:
                add("z", "z" + ("+" if tree == 2 else "-"), ("own", 0, 0), [])
                for k, (z, par) in enumerate((("own", []), ("other", ["z"]))):
                    add(f"p+{z}", fast + "+", (z, 0, 0), par)
                    add(f"p-{z}", fast + "-", (z, 0, 0), par)
                    a = "+" if k else "-"
                    add(f"p2{z}", fast + a, (z, -1 if a == "+" else 1, 0), [f"p{a}{z}"])
                arrived = {
                    0: ["z"],
                    -1: ["p+own", "p+other"],
                    1: ["p-own", "p-other"],
                    2: ["p2own", "p2other"],
                }
                for k, r in enumerate((0, -1, 1, 2)):
                    add(f"q+{r}", slow + "+", ("both", r, 0), arrived[r])
                    add(f"q-{r}", slow + "-", ("both", r, 0), arrived[r])
                    a = "+" if (k + flip) % 2 else "-"
                    add(f"q2{r}", slow + a, ("both", r, -1 if a == "+" else 1), [f"q{a}{r}"])
    return edges


def landing(edge):
    z, y, x = edge["region"]
    shift = 1 if edge["way"][1] == "+" else -1
    if edge["way"][0] == "z":
        return {"own": "other", "other": "own", "both": "both"}[z], y, x
    wrap = {-2: 2, 3: -1}
    if edge["way"][0] == "y":
        return z, wrap.get(y - shift, y - shift), x
    return z, y, wrap.get(x - shift, x - shift)


def unit_of(edge):
    group, tree, name = edge["key"]
    if tree < 2 and name[0] == "z":
        return (group, tree, "z", landing(edge)[1]) if group == DOWN else (group, tree, "z")
    if tree >= 2 and name[:2] == "q2" and (group != DOWN or tree == 2):
        return (group, tree, "q2")
    return edge["key"]


def in_row(edge, row):
    z, y, _ = landing(edge)
    return z in (row[0], "both") and y == row[1]


def planned(edges):
    index = {e["key"]: k for k, e in enumerate(edges)}
    free, landed, begun = {}, {}, {}
    waiting, order = list(range(len(edges))), []
    while waiting:
        best = None
        for k in waiting:
            e = edges[k]
            if any(index[p] not in landed for p in e["parents"]):
                continue
            ready = max([landed[index[p]] for p in e["parents"]], default=0.0)
            start = max(ready, free.get(e["way"], 0.0))
            if best is None or (start, e["key"][0], ready) < best[0]:
                best = ((start, e["key"][0], ready), k, ready, start)
        _, k, ready, start = best
        free[edges[k]["way"]] = start + edges[k]["bytes"] / LINK_RATE
        landed[k] = free[edges[k]["way"]] + HOP_US
        begun[k] = (ready, start)
        waiting.remove(k)
        order.append(k)
    last, due = {}, {}
    for k in order:
        due[k] = max(begun[k][0], begun[k][1] - EARLY_US, last.get(edges[k]["way"], 0.0))
        last[edges[k]["way"]] = due[k]
    order.sort(key=lambda k: (due[k], begun[k][1]))
    return index, order, landed, due


def send_unit(edge):
    group, tree, name = edge["key"]
    return (group * 4 + tree) * 3 + "pqz".index(name[0])


class Gather:
    def __init__(self, edges, plan, buffers, send, recv):
        self.edges, self.buffers, self.send, self.recv = edges, buffers, send, recv
        self.index, self.order, self.landed, self.due = plan
        self.seen, self.queue = set(), list(self.order)
        self.unit = {}
        for e in edges:
            self.unit.setdefault(unit_of(e), len(self.unit))
        fs, rep = lax.axis_index("fs"), lax.axis_index("rep")
        x, y, half = lax.rem(fs, 4), lax.rem(lax.div(fs, 4), 4), lax.div(fs, 16)
        z = rep * 2 + half
        self.x = {r: (lax.rem(x + r + 4, 4) if r else x) for r in (-1, 0, 1, 2)}
        self.y = {r: (lax.rem(y + r + 4, 4) if r else y) for r in (-1, 0, 1, 2)}
        self.z = {"own": half, "other": 1 - half}
        self.device = {}
        for sign, d in (("+", 1), ("-", -1)):
            self.device["x" + sign] = {"fs": half * 16 + y * 4 + self.x[d]}
            self.device["y" + sign] = {"fs": half * 16 + self.y[d] * 4 + x}
            beyond = lax.rem(z + d + 4, 4)
            self.device["z" + sign] = {
                "rep": lax.div(beyond, 2),
                "fs": lax.rem(beyond, 2) * 16 + y * 4 + x,
            }

    def place(self, edge, arriving):
        z, y, x = landing(edge) if arriving else edge["region"]
        at_z = pl.ds(0, 2) if z == "both" else self.z[z]
        start, width = edge["columns"]
        return self.buffers[edge["buffer"]].at[
            at_z, self.y[y], self.x[x], :, pl.ds(start, width)
        ]

    def copy(self, k, arriving):
        edge = self.edges[k]
        ref = self.place(edge, arriving)
        return pltpu.make_async_remote_copy(
            src_ref=ref,
            dst_ref=ref,
            send_sem=self.send.at[send_unit(edge)],
            recv_sem=self.recv.at[self.unit[unit_of(edge)]],
            device_id=self.device[edge["way"]],
            device_id_type=MESH,
        )

    def whole(self, edge, at):
        start, width = edge["columns"]
        ref = self.buffers[edge["buffer"]].at[(*at, slice(None), pl.ds(start, width))]
        return pltpu.make_async_remote_copy(
            src_ref=ref,
            dst_ref=ref,
            send_sem=self.send.at[send_unit(edge)],
            recv_sem=self.recv.at[self.unit[unit_of(edge)]],
            device_id=self.device[edge["way"]],
            device_id_type=MESH,
        )

    def wait_unit(self, k):
        edge = self.edges[k]
        unit, every = unit_of(edge), pl.ds(0, 4)
        if unit == edge["key"]:
            self.copy(k, True).wait_recv()
        elif unit[2] == "z":
            self.whole(edge, (self.z["other"], self.y[unit[3]] if len(unit) > 3 else every, every)).wait_recv()
        elif unit[1] == 2:
            self.whole(edge, (pl.ds(0, 2), self.y[2], every)).wait_recv()
        else:
            self.whole(edge, (pl.ds(0, 2), every, self.x[2])).wait_recv()

    def arrivals(self, ks):
        found = []
        for k in ks:
            unit = unit_of(self.edges[k])
            if unit not in self.seen:
                self.seen.add(unit)
                found.append((True, k))
        return found

    def begin(self, k):
        return self.arrivals([self.index[p] for p in self.edges[k]["parents"]]) + [(False, k)]

    def due_by(self, until):
        steps = []
        while self.queue and self.due[self.queue[0]] <= until:
            steps += self.begin(self.queue.pop(0))
        return steps

    def members(self, group):
        return [k for k in self.order if self.edges[k]["key"][0] == group]

    def run(self, steps):
        for arriving, k in steps:
            if arriving:
                self.wait_unit(k)
            else:
                self.copy(k, False).start()

    def pump(self, until):
        self.run(self.due_by(until))

    def until_done(self, group, row=None):
        members = self.members(group)
        if row is not None:
            members = [k for k in members if in_row(self.edges[k], row)]
        steps = self.due_by(max([self.landed[k] for k in members], default=0.0) - HOP_US)
        while any(k in self.queue for k in members) or any(
            self.index[p] in self.queue for k in members for p in self.edges[k]["parents"]
        ):
            steps += self.begin(self.queue.pop(0))
        return steps + self.arrivals(members)

    def group_done(self, group):
        self.run(self.until_done(group))

    def group_time(self, group):
        return max([self.landed[k] for k in self.members(group)], default=0.0)

    def timetable(self, count, first, pace, subs=1):
        return [
            [self.due_by(first + pace * (k + j / subs)) for j in range(subs)] for k in range(count)
        ]

    def sent(self, group):
        done = set()
        for k in self.members(group):
            edge = self.edges[k]
            tree, level = edge["key"][1], edge["key"][2][0]
            if send_unit(edge) in done:
                continue
            done.add(send_unit(edge))
            half, y, x = self.z["own"], self.y[0], self.x[0]
            if tree < 2:
                at = {"p": (half, y, pl.ds(0, 3)), "q": (half, pl.ds(0, 3), pl.ds(0, 4)), "z": (half, pl.ds(0, 4), pl.ds(0, 4))}
            else:
                at = {"z": (half, y, x), "p": (pl.ds(0, 2), y, pl.ds(0, 3)), "q": (pl.ds(0, 2), pl.ds(0, 3), pl.ds(0, 4))}
            self.whole(edge, at[level]).wait_send()


def at_step(step, table, gather, sub=0):
    for k, steps in enumerate(table):
        if steps[sub]:

            @pl.when(step == k)
            def _(steps=steps[sub]):
                gather.run(steps)


def shifted_down(values, amount, fill, row):
    return jnp.where(row >= amount, pltpu.roll(values, amount, 0), fill)


def scan_rows(decay, driven, row):
    rows = decay.shape[0]
    step = 1
    while step < rows:
        before_b = shifted_down(driven, step, 0.0, row)
        before_a = shifted_down(decay, step, 1.0, row)
        driven = decay * before_b + driven
        decay = decay * before_a
        step *= 2
    return decay, driven


LEN = 768
BLOCK = 128
ROWS = 256
NORM_ROWS = 32


def kernel(edges, plan, *refs):
    (x, gain, lin, branch, taps, rate, admit, logit, mix_gain, out_w, ffn_gain, gate, up, gate_taps, up_taps, down) = refs[:16]
    result = refs[16]
    small = (gain, taps, rate, admit, logit, mix_gain, ffn_gain, gate_taps, up_taps)
    held = refs[17 : 17 + len(small)]
    (b0, b1, b2, b3, full, normed, mixed, sent, got, hidden, dgot, final, pad_a, pad_b) = refs[26:40]
    (send, recv, load, ssem, xsem, osend, orecv, dsend, drecv, fsem) = refs[40:]
    tp = lax.axis_index("tp")
    gather = Gather(edges, plan, (b0, b1, b2, b3), send, recv)
    partner = {"tp": 1 - tp}
    zl, y0, x0 = gather.z["own"], gather.y[0], gather.x[0]

    x_load = pltpu.make_async_copy(x, full.at[tp], load.at[0])
    small_loads = [pltpu.make_async_copy(a, b, ssem.at[k]) for k, (a, b) in enumerate(zip(small, held))]
    (gain, taps, rate, admit, logit, mix_gain, ffn_gain, gate_taps, up_taps) = held
    loads = []
    pieces = [(out_w, b1, 2, 0, 0, 1024), (down, b3, 4, 0, 0, 1408)]
    for k in range(8):
        pieces += [(lin, b0, 1, k * 128, k * 256, 128), (branch, b0, 1, k * 128, k * 256 + 128, 128)]
    for k in range(11):
        pieces += [(gate, b2, 3, k * 128, k * 256, 128), (up, b2, 3, k * 128, k * 256 + 128, 128)]
    for source, target, owner, at, to, width in pieces:
        loads.append(
            pltpu.make_async_copy(
                source.at[:, pl.ds(at, width)], target.at[zl, y0, x0, :, pl.ds(to, width)], load.at[owner]
            )
        )
    for one in loads:
        one.start()
    barrier = pltpu.get_barrier_semaphore()
    for device in [*gather.device.values(), partner]:
        pl.semaphore_signal(barrier, inc=1, device_id=device, device_id_type=MESH)
    pl.semaphore_wait(barrier, 7)
    x_copy = pltpu.make_async_remote_copy(
        src_ref=x, dst_ref=full.at[tp], send_sem=xsem.at[0], recv_sem=xsem.at[1], device_id=partner, device_id_type=MESH
    )
    for k, buffer in enumerate((b0, b1, b2, b3)):
        slot = buffer.at[zl, y0, x0]
        pltpu.make_async_copy(slot, slot, load.at[k + 1]).wait()
    gather.pump(0.0)
    x_copy.start()
    x_load.start()
    for one in small_loads:
        one.start()
    gather.pump(LEAD_US)
    x_load.wait()
    for one in small_loads:
        one.wait()
    x_copy.wait_send()
    pltpu.make_async_remote_copy(
        src_ref=x, dst_ref=full.at[1 - tp], send_sem=xsem.at[0], recv_sem=xsem.at[1], device_id=partner, device_id_type=MESH
    ).wait_recv()

    def norm(chunk, scales, with_sums):
        rows = pl.ds(pl.multiple_of(chunk * NORM_ROWS, NORM_ROWS), NORM_ROWS)
        halves = []
        for h in range(2):
            part = full[h, rows, :].astype(F32)
            if with_sums:
                extra = [
                    sent[h, q, rows, :].astype(F32) + got[h, q, rows, :].astype(F32) for q in range(4)
                ]
                rounded = (part + jnp.concatenate(extra, axis=1)).astype(BF16)
                full[h, rows, :] = rounded
                part = rounded.astype(F32)
            halves.append(part)
        total = sum(jnp.sum(part * part, axis=-1, keepdims=True) for part in halves)
        factor = lax.rsqrt(total * (1.0 / 2048.0) + EPS)
        for h in range(2):
            normed[rows, h * 1024 : h * 1024 + 1024] = (halves[h] * factor * scales[:, h * 1024 : h * 1024 + 1024]).astype(BF16)

    table = gather.timetable(LEN // NORM_ROWS // 3, *NORM_PACE)

    @pl.loop(0, LEN // NORM_ROWS // 3)
    def _(part):
        at_step(part, table, gather)

        @pl.loop(0, 3)
        def _(chunk):
            norm(part * 3 + chunk, gain, False)

    pad_a[0:8, :] = jnp.zeros((8, BLOCK), F32)
    pad_b[0:8, :] = jnp.zeros((8, BLOCK), F32)
    row = lax.broadcasted_iota(jnp.int32, (ROWS, BLOCK), 0)
    gather.group_done(0)
    start = gather.group_time(0)

    def both(buffer, step):
        columns = pl.ds(pl.multiple_of(step * 256, 256), 256)
        weights = buffer[:, :, :, :, columns].reshape(2048, 256)
        total = jnp.dot(normed[...], weights, preferred_element_type=F32)
        return total.astype(BF16).astype(F32)

    table1 = gather.timetable(8, start + MIX_PACE[0], MIX_PACE[1], 4)

    @pl.loop(0, 8)
    def _(step):
        at_step(step, table1, gather, 0)
        lanes = pl.ds(pl.multiple_of(step * BLOCK, BLOCK), BLOCK)
        values = both(b0, step)
        pad_a[8 : 8 + LEN, :] = values[:, :BLOCK]
        pad_b[8 : 8 + LEN, :] = values[:, BLOCK:]
        tap = taps[:, lanes]
        base = -GATE_SCALE * jax.nn.softplus(-logit[:, lanes])
        scale = mix_gain[:, lanes]
        carry = jnp.zeros((1, BLOCK), F32)
        for c in range(LEN // ROWS):
            at_step(step, table1, gather, c + 1)
            at = c * ROWS
            filtered = sum(pad_a[5 + j + at : 5 + j + at + ROWS, :] * tap[j : j + 1, :] for j in range(4))
            rounded = filtered.astype(BF16)
            rate_gate = jax.nn.sigmoid(jnp.dot(rounded, rate[step], preferred_element_type=F32))
            admitted = jax.nn.sigmoid(jnp.dot(rounded, admit[step], preferred_element_type=F32))
            log_decay = rate_gate * base
            decay = jnp.exp(log_decay)
            rest = -jnp.tanh(log_decay) * (1.0 + decay * decay)
            driven = jnp.sqrt(rest) * admitted * filtered
            product, states = scan_rows(decay, driven, row)
            states = states + product * carry
            carry = states[ROWS - 1 : ROWS, :]
            gated = states * jax.nn.gelu(pad_b[8 + at : 8 + at + ROWS, :], approximate=True)
            mean = jnp.mean(gated * gated, axis=-1, keepdims=True)
            mixed[at : at + ROWS, lanes] = (gated * lax.rsqrt(mean + EPS) * scale).astype(BF16)

    gather.group_done(1)

    def out_copy(j):
        h, q = lax.rem(1 - tp + lax.div(j, 4), 2), lax.rem(j, 4)
        return pltpu.make_async_remote_copy(
            src_ref=sent.at[h, q], dst_ref=got.at[h, q], send_sem=osend.at[j], recv_sem=orecv.at[j],
            device_id=partner, device_id_type=MESH,
        )

    def arriving_copy(j):
        h, q = lax.rem(tp + lax.div(j, 4), 2), lax.rem(j, 4)
        return pltpu.make_async_remote_copy(
            src_ref=sent.at[h, q], dst_ref=got.at[h, q], send_sem=osend.at[j], recv_sem=orecv.at[j],
            device_id=partner, device_id_type=MESH,
        )

    table2 = gather.timetable(8, start + OUT_PACE[0], OUT_PACE[1])

    @pl.loop(0, 8)
    def _(j):
        at_step(j, table2, gather)
        h, q = lax.rem(1 - tp + lax.div(j, 4), 2), lax.rem(j, 4)
        weights = b1[h, q].reshape(256, 1024)
        part = lax.dot_general(mixed[...], weights, (((1,), (1,)), ((), ())), preferred_element_type=F32)
        sent[h, q] = part.astype(BF16)

        @pl.when(j > 0)
        def _():
            out_copy(j - 1).start()

    out_copy(7).start()
    gather.pump(start + NORM2_US)
    for j in range(8):
        arriving_copy(j).wait_recv()

    table3 = gather.timetable(LEN // NORM_ROWS // 3, start + NORM2_US, NORM_PACE[1])

    @pl.loop(0, LEN // NORM_ROWS // 3)
    def _(part):
        at_step(part, table3, gather)

        @pl.loop(0, 3)
        def _(chunk):
            norm(part * 3 + chunk, ffn_gain, True)

    for j in range(8):
        out_copy(j).wait_send()
    gather.sent(0)
    gather.group_done(GATE_UP[0])
    ready = gather.group_time(GATE_UP[0])
    table4 = gather.timetable(6, ready + FFN_PACE[0], FFN_PACE[1], 2)
    middle = gather.until_done(GATE_UP[1])
    later = max(ready + 6 * FFN_PACE[1], gather.group_time(GATE_UP[1])) + FFN_PACE[0]
    table5 = gather.timetable(5, later, FFN_PACE[1], 2)
    table4 = table4 + [[middle + table5[0][0], table5[0][1]]] + table5[1:]

    @pl.loop(0, 11)
    def _(step):
        at_step(step, table4, gather, 0)
        lanes = pl.ds(pl.multiple_of(step * BLOCK, BLOCK), BLOCK)
        values = both(b2, step)
        pad_a[8 : 8 + LEN, :] = values[:, :BLOCK]
        pad_b[8 : 8 + LEN, :] = values[:, BLOCK:]
        at_step(step, table4, gather, 1)
        tap_g, tap_u = gate_taps[:, lanes], up_taps[:, lanes]
        for c in range(LEN // ROWS):
            at = c * ROWS
            conv_g = sum(pad_a[6 + j + at : 6 + j + at + ROWS, :] * tap_g[j : j + 1, :] for j in range(3))
            conv_u = sum(pad_b[6 + j + at : 6 + j + at + ROWS, :] * tap_u[j : j + 1, :] for j in range(3))
            hidden[at : at + ROWS, lanes] = (jax.nn.silu(conv_g) * conv_u).astype(BF16)

    tables = [[gather.until_done(DOWN, row)] for row in ROW_ORDER]

    def row_of(j):
        k = lax.rem(j, 4)
        step = jnp.where(k == 2, 3, jnp.where(k == 3, 2, k))
        return lax.rem(zl + lax.div(j, 4), 2), lax.rem(y0 + step, 4)

    def down_copy(q):
        return pltpu.make_async_remote_copy(
            src_ref=sent.at[0, q], dst_ref=dgot.at[q], send_sem=dsend.at[q], recv_sem=drecv.at[q],
            device_id=partner, device_id_type=MESH,
        )

    def final_copy(q):
        lanes = pl.ds(pl.multiple_of(q * 256, 256), 256)
        return pltpu.make_async_copy(final.at[:, lanes], result.at[:, lanes], fsem.at[q])

    def complete(j):
        _, q = row_of(j)
        down_copy(q).wait_recv()
        lanes = pl.ds(pl.multiple_of(q * 256, 256), 256)
        total = sent[1, q].astype(F32) + dgot[q].astype(F32)
        final[:, lanes] = (full[tp, :, lanes].astype(F32) + total).astype(BF16)
        final_copy(q).start()

    def pass_on(j):
        h, q = row_of(j)

        @pl.when(h != tp)
        def _():
            down_copy(q).start()

    @pl.loop(0, 8)
    def _(j):
        at_step(j, tables, gather)
        h, q = row_of(j)
        weights = b3[h, q].reshape(256, 1408)
        part = lax.dot_general(hidden[...], weights, (((1,), (1,)), ((), ())), preferred_element_type=F32)
        sent[jnp.where(h == tp, 1, 0), q] = part.astype(BF16)

        @pl.when(j > 0)
        def _():
            pass_on(j - 1)

        @pl.when(j >= 6)
        def _():
            complete(j - 6)

    pass_on(7)
    gather.pump(1e9)
    for group in range(1, DOWN):
        gather.sent(group)
    complete(2)
    complete(3)
    gather.sent(DOWN)
    for q in range(4):
        down_copy(q).wait_send()
        final_copy(q).wait()


LEAD_US = 3.0
NORM_PACE = (3.0, 0.9)
MIX_PACE = (4.0, 3.0)
OUT_PACE = (28.0, 0.8)
NORM2_US = 37.0
FFN_PACE = (3.0, 1.4)


def local(
    stream_in, mix_gain, lin_weight, branch_weight, lin_taps, rate_blocks, admit_blocks, decay_logit, mix_out_gain,
    out_weight, ffn_gain, gate_weight, up_weight, gate_taps, up_taps, down_weight,
):
    edges = tree_edges()
    plan = planned(edges)
    count, sends = len({unit_of(e) for e in edges}), 12 * len(GROUPS)
    any_space = pl.BlockSpec(memory_space=pl.ANY)
    operands = [
        stream_in[0],
        mix_gain.reshape(1, 2048),
        lin_weight,
        branch_weight,
        lin_taps,
        rate_blocks,
        admit_blocks,
        decay_logit.reshape(1, 1024),
        mix_out_gain.reshape(1, 1024),
        out_weight.T,
        ffn_gain.reshape(1, 2048),
        gate_weight,
        up_weight,
        gate_taps,
        up_taps,
        down_weight.T,
    ]
    small = [operands[k] for k in (1, 4, 5, 6, 7, 8, 10, 13, 14)]
    dma = pltpu.SemaphoreType.DMA
    result = pl.pallas_call(
        functools.partial(kernel, edges, plan),
        out_shape=jax.ShapeDtypeStruct((LEN, 1024), BF16),
        in_specs=[any_space] * len(operands),
        out_specs=any_space,
        scratch_shapes=[
            *[pltpu.VMEM(a.shape, a.dtype) for a in small],
            pltpu.VMEM((2, 4, 4, SHARD_ROWS, 2048), BF16),
            pltpu.VMEM((2, 4, 4, SHARD_ROWS, 1024), BF16),
            pltpu.VMEM((2, 4, 4, SHARD_ROWS, 2816), BF16),
            pltpu.VMEM((2, 4, 4, SHARD_ROWS, 1408), BF16),
            pltpu.VMEM((2, LEN, 1024), BF16),
            pltpu.VMEM((LEN, 2048), BF16),
            pltpu.VMEM((LEN, 1024), BF16),
            pltpu.VMEM((2, 4, LEN, 256), BF16),
            pltpu.VMEM((2, 4, LEN, 256), BF16),
            pltpu.VMEM((LEN, 1408), BF16),
            pltpu.VMEM((4, LEN, 256), BF16),
            pltpu.VMEM((LEN, 1024), BF16),
            pltpu.VMEM((LEN + 8, BLOCK), F32),
            pltpu.VMEM((LEN + 8, BLOCK), F32),
            dma((sends,)), dma((count,)), dma((5,)), dma((len(small),)), dma((2,)), dma((8,)), dma((8,)), dma((4,)), dma((4,)),
            dma((4,)),
        ],
        compiler_params=pltpu.CompilerParams(
            collective_id=0, has_side_effects=True, vmem_limit_bytes=63 * 1024 * 1024
        ),
    )(*operands)
    return result[None]


def solution(mesh):
    placed = (
        P(("rep", "fs"), None, "tp"), P(), P("fs", "tp"), P("fs", "tp"), P(None, "tp"), P("tp", None, None),
        P("tp", None, None), P("tp"), P("tp"), P("tp", "fs"), P(), P("fs", "tp"), P("fs", "tp"), P(None, "tp"),
        P(None, "tp"), P("tp", "fs"),
    )
    return jax.shard_map(
        local, mesh=mesh, in_specs=placed, out_specs=P(("rep", "fs"), None, "tp"), check_vma=False
    )
```
